32 devices in a mesh: fs: 8 (over z, y), tp: 4 (over x, core).
Axes of the slice: x: 2, y: 2, z: 4, core: 2. Of those that a mesh axis runs over, the one named last changes fastest.
Arguments:
- tokens: bfloat16 [512, 2048], P('fs', 'tp'), may hold values from -6 to 6
- norm_gain: float32 [2048], P('fs'), may hold values from 0.1 to 1.9
- gate_weight: float32 [8, 2048, 512], P(None, 'fs', 'tp'), may hold values from -0.125 to 0.125
- up_weight: float32 [8, 2048, 512], P(None, 'fs', 'tp'), may hold values from -0.125 to 0.125
- down_weight: float32 [8, 2048, 512], P(None, 'fs', 'tp'), may hold values from -0.25 to 0.25
- route_ids: int32 [512, 2], P('fs'), may hold values from 0 to 7, all different within a row; in each aligned block of 64 rows (0 to 63, 64 to 127, ...) at most 24 rows name the same one
- group_weight: float32 [512], P('fs'), may hold values from 0.3 to 1
- logit_gap: float32 [512], P('fs'), may hold values from -6 to 6
Outputs:
- gate_new: bfloat16 [8, 2048, 512], P('fs', None, 'tp')
- up_new: bfloat16 [8, 2048, 512], P('fs', None, 'tp')
- down_new: bfloat16 [8, 2048, 512], P('fs', None, 'tp')
- mixed: bfloat16 [512, 2048], P('fs', 'tp')
The draws below stay inside these ranges and needn't reach their ends.
Inputs may be any that keep to these rules, and one draw needn't show every extreme that they name: `route_ids`: each row names two different experts. In the rows of one device no expert is named by more than 24 rows, a bound that some block reaches.
All inputs are finite; a program needn't handle non-finite values.
Results may differ from the reference program's by a relative error of at most 0.011.
Values may be sent and summed in bfloat16 or wider, within the bound.
No kernel may reach another device: no remote copies, remote signals or barrier semaphores. Data moves between devices by JAX's collectives and lax.ppermute only.
A program may use at most 64 MiB of HBM per device.

```python
import math
import jax
import jax.numpy as jnp
import numpy as np
from jax import lax

D = 2048
FF = 512
TOK_DEV = 64
EXPERTS = 8
CAP = 24
TOKENS = 512
N_FS = 8
N_TP = 4


def block_scale(stream_key, shape, cuts, low, high):
    factor_of = 1.0
    for axis_at, parts in cuts:
        heights = jax.random.uniform(jax.random.fold_in(jax.random.fold_in(stream_key, 6), axis_at), (parts,), jnp.float32, low / len(cuts), high / len(cuts))
        factor_of = factor_of * jnp.repeat(jnp.exp(heights), shape[axis_at] // parts).reshape((-1,) + (1,) * (len(shape) - 1 - axis_at))
    return factor_of


def routed_block(rng, own, number, rows, amount, top, most, slope):
    order = jax.random.permutation(rng, amount)
    heavy_load, ordinary = load_shares(amount, rows * top, most, slope, True), load_shares(amount, rows * top, most, slope, False)
    places = jnp.arange(amount)

    def named(tallies, offset_by):
        used = int((tallies > 0).sum())
        fixed = max(1, used // 4)
        passed = fixed + (places - fixed + offset_by * (used - fixed)) % max(1, amount - fixed)
        return jnp.zeros((amount,), jnp.int32).at[order[jnp.where(places < fixed, places, passed)]].set(jnp.asarray(tallies, jnp.int32))

    tallies = jnp.where(number % 4 == 0, named(heavy_load, number // 4), named(ordinary, number - number // 4 - 1))
    mixed = jax.random.permutation(jax.random.fold_in(own, 3), amount)
    source_of, receiver = mixed[0:amount // 2 * 2:2], mixed[1:amount // 2 * 2:2]
    slack = jnp.minimum(tallies[source_of] - 1, most - tallies[receiver]) // 2
    slack = jnp.where((source_of == order[0]) | (receiver == order[0]) | (tallies[receiver] == 0), 0, jnp.maximum(slack, 0))
    passed = jax.random.randint(jax.random.fold_in(own, 4), (amount // 2,), 0, 1 << 20) % (slack + 1)
    tallies = tallies.at[source_of].add(-passed).at[receiver].add(passed)
    items = jnp.searchsorted(jnp.cumsum(tallies), jnp.arange(rows * top), side="right").astype(jnp.int32)
    table = items.reshape(top, rows).T
    table = table[jax.random.permutation(jax.random.fold_in(own, 1), rows)]
    offset_by = jax.random.randint(jax.random.fold_in(own, 2), (rows, 1), 0, top)
    return jnp.take_along_axis(table, (jnp.arange(top)[None, :] + offset_by) % top, axis=1)


def load_shares(number_of, total, reach, lean, full):
    portions = [(1 << 20) // math.isqrt(grade ** lean) + 1 for grade in range(1, number_of + 1)]
    largest = reach if full else min(reach, max(-(-total // number_of), total * portions[0] // sum(portions)))
    least = 1 if total - largest >= number_of - 1 else 0
    counts, spare = [largest] + [least] * (number_of - 1), total - largest - least * (number_of - 1)
    while spare > 0:
        movable = [i for i in range(1, number_of) if counts[i] < largest] or [i for i in range(1, number_of) if counts[i] < reach]
        pool, budget = sum([portions[i] for i in movable]), spare
        for i in movable:
            extra = min(reach - counts[i], max(1, budget * portions[i] // pool), spare)
            counts[i] = counts[i] + extra
            spare = spare - extra
    return np.array(counts)


def centred(rng, dims, width, most, cuts=(), kind=jnp.bfloat16):
    drawn = jax.random.normal(rng, dims, jnp.float32) * width
    if len(cuts) > 0:
        drawn = block_scale(rng, dims, cuts, -0.22, 0.18) * drawn
    return jnp.clip(drawn, min=-most, max=most).astype(kind)


def setup_inputs(seed: int = 0) -> dict:
    arg_keys = jax.random.split(jax.random.key(seed), 9)
    tokens = centred(arg_keys[0], (TOKENS, D), 1.0, 6.0, ((0, 8), (1, 4)))
    norm_gain = jnp.clip(1.0 + 0.18 * jax.random.normal(arg_keys[1], (D,), jnp.float32), 0.1, 1.9)
    gate_weight = centred(arg_keys[2], (EXPERTS, D, FF), D ** -0.5, 0.125, ((1, 8), (2, 4)), jnp.float32)
    up_weight = centred(arg_keys[3], (EXPERTS, D, FF), D ** -0.5, 0.125, ((1, 8), (2, 4)), jnp.float32)
    down_weight = centred(arg_keys[4], (EXPERTS, D, FF), FF ** -0.5, 0.25, ((1, 8), (2, 4)), jnp.float32)
    route_ids_keys = jax.random.split(jax.random.fold_in(arg_keys[5], 1), TOKENS // TOK_DEV)
    route_ids_turns = jax.random.permutation(jax.random.fold_in(arg_keys[5], 3), TOKENS // TOK_DEV)
    route_ids = jax.vmap(lambda own, number: routed_block(jax.random.fold_in(arg_keys[5], 2), own, number, TOK_DEV, EXPERTS, 2, CAP, 2))(route_ids_keys, route_ids_turns).reshape((TOKENS, 2))
    group_weight = jnp.clip(0.3 + 0.7 * jax.random.uniform(arg_keys[6], (TOKENS,), jnp.float32) ** block_scale(arg_keys[6], (TOKENS,), ((0, 8),), -0.2, 0.2), 0.3, 1.0)
    logit_gap = centred(arg_keys[7], (TOKENS,), 1.5, 6.0, ((0, 8),), jnp.float32)
    return dict(tokens=tokens, norm_gain=norm_gain, gate_weight=gate_weight, up_weight=up_weight, down_weight=down_weight, route_ids=route_ids, group_weight=group_weight, logit_gap=logit_gap)


def reference(tokens, norm_gain, gate_weight, up_weight, down_weight, route_ids, group_weight, logit_gap):
    scaled = norm_gain.astype(jnp.float32)[None, :, None]
    gate_new = (gate_weight * scaled).astype(jnp.bfloat16)
    up_new = (up_weight * scaled).astype(jnp.bfloat16)
    down_new = down_weight.astype(jnp.bfloat16)
    pair_count = 2 * TOK_DEV
    flat_ids = route_ids.reshape(N_FS, pair_count).astype(jnp.int32)
    onehot = (flat_ids[:, :, None] == jnp.arange(EXPERTS, dtype=jnp.int32)[None, None, :]).astype(jnp.float32)
    before = jnp.cumsum(onehot, axis=1) - onehot
    ranked = jnp.sum(before * onehot, axis=2).astype(jnp.int32)
    slot_ids = flat_ids * CAP + ranked
    owners = jnp.broadcast_to((jnp.arange(pair_count, dtype=jnp.int32) // 2)[None, :], (N_FS, pair_count))
    blocks = jnp.broadcast_to(jnp.arange(N_FS, dtype=jnp.int32)[:, None], (N_FS, pair_count))
    slot_table = jnp.full((N_FS, EXPERTS * CAP), TOK_DEV, jnp.int32).at[blocks, slot_ids].set(owners)
    padded = jnp.concatenate([tokens.reshape(N_FS, TOK_DEV, D), jnp.zeros((N_FS, 1, D), jnp.bfloat16)], axis=1)
    source_ids = jnp.arange(N_FS, dtype=jnp.int32)[:, None]

    def one_expert(expert):
        picked = lax.dynamic_slice_in_dim(slot_table, expert * CAP, CAP, 1)
        slot_rows = padded[source_ids, picked].reshape(N_FS * CAP, D)
        gate_acc = jnp.dot(slot_rows, gate_new[expert], preferred_element_type=jnp.float32)
        up_acc = jnp.dot(slot_rows, up_new[expert], preferred_element_type=jnp.float32)
        hidden = (jax.nn.silu(gate_acc) * up_acc).astype(jnp.bfloat16)
        pieces = hidden.reshape(N_FS * CAP, N_TP, FF // N_TP).astype(jnp.float32)
        down_pieces = down_new[expert].reshape(D, N_TP, FF // N_TP).astype(jnp.float32)
        partial_value = jnp.einsum('rjf,djf->jrd', pieces, down_pieces).astype(jnp.bfloat16)
        partial_value = lax.optimization_barrier(partial_value)
        summed = jnp.sum(partial_value.astype(jnp.float32), axis=0).astype(jnp.bfloat16)
        return summed.reshape(N_FS, CAP, D)

    outputs = lax.map(one_expert, jnp.arange(EXPERTS, dtype=jnp.int32))
    gathered = outputs[flat_ids, blocks, ranked].reshape(TOKENS, 2, D).astype(jnp.float32)
    gap = logit_gap.astype(jnp.float32)
    first_weight = group_weight * jax.nn.sigmoid(gap)
    second_weight = group_weight * jax.nn.sigmoid(-gap)
    mixed = (first_weight[:, None] * gathered[:, 0] + second_weight[:, None] * gathered[:, 1]).astype(jnp.bfloat16)
    return gate_new, up_new, down_new, mixed
```

```python
import functools

import jax
import jax.numpy as jnp
from jax import lax
from jax.experimental import pallas as pl
from jax.experimental.pallas import tpu as pltpu
from jax.sharding import PartitionSpec as P

BF16 = jnp.bfloat16
F32 = jnp.float32


GRANT = pltpu.CompilerParams(vmem_limit_bytes=8 * 1024 * 1024)
VMEM = pltpu.VMEM
ANY = pl.ANY


def whole(space):
    return pl.BlockSpec(memory_space=space)


def column(row):
    n = row.shape[1]
    same = lax.broadcasted_iota(jnp.int32, (n, n), 0) == lax.broadcasted_iota(jnp.int32, (n, n), 1)
    return jnp.sum(jnp.where(same, row, 0.0), axis=1, keepdims=True)


def own_places():
    return lax.axis_index("fs").astype(jnp.int32), lax.axis_index("tp").astype(jnp.int32)


def cast_chunks(picks, gain, weights):
    count, stack = len(picks), len(weights)
    rows, cols = weights[0].shape[1:]
    scaled = gain is not None

    def kernel(*refs):
        gain_refs = refs[: int(scaled)]
        at = int(scaled)
        sources = refs[at : at + stack]
        targets = refs[at + stack : at + stack + count]
        buffer, sems = refs[at + stack + count :]
        own, lane = own_places()
        copies = []
        for n in range(count):
            for w in range(stack):
                copy = pltpu.make_async_copy(
                    sources[w].at[picks[n](own, lane)], buffer.at[n, w], sems.at[n, w]
                )
                copy.start()
                copies.append((n, w, copy))
        factor = column(gain_refs[0][...]) if scaled else None
        for n, w, copy in copies:
            copy.wait()
            value = buffer[n, w]
            if scaled:
                value = value * factor
            targets[n][w] = value.astype(BF16)

    return pl.pallas_call(
        kernel,
        in_specs=[whole(VMEM)] * int(scaled) + [whole(ANY)] * stack,
        out_specs=[whole(VMEM)] * count,
        out_shape=[jax.ShapeDtypeStruct((stack, rows, cols), BF16)] * count,
        scratch_shapes=[
            VMEM((count, stack, rows, cols), F32),
            pltpu.SemaphoreType.DMA((count, stack)),
        ],
        compiler_params=GRANT,
        name="cast_chunks",
    )(*([gain] if scaled else []), *weights)


def dispatch_rows(routes, group_weight, logit_gap, tokens, experts, capacity):
    rows, features = tokens.shape

    def kernel(route_ref, group_ref, gap_ref, tok_ref, info_ref, *outs):
        own, _ = own_places()
        first = route_ref[0:1, :]
        second = route_ref[1:2, :]
        names = lax.broadcasted_iota(jnp.int32, (experts, rows), 0)
        hit_first = (names == first).astype(F32)
        hit_second = (names == second).astype(F32)
        above = lax.broadcasted_iota(jnp.int32, (rows, rows), 0) < lax.broadcasted_iota(
            jnp.int32, (rows, rows), 1
        )
        before = jnp.dot(
            (hit_first + hit_second).astype(BF16),
            above.astype(F32).astype(BF16),
            preferred_element_type=F32,
        )
        rank_first = jnp.sum(before * hit_first, axis=0, keepdims=True)
        rank_second = jnp.sum(before * hit_second, axis=0, keepdims=True)
        pos_first = (first ^ own) * capacity + rank_first.astype(jnp.int32)
        pos_second = (second ^ own) * capacity + rank_second.astype(jnp.int32)
        slots = lax.broadcasted_iota(jnp.int32, (experts * capacity, rows), 0)
        chosen = ((pos_first == slots) | (pos_second == slots)).astype(F32).astype(BF16)
        outgoing = jnp.dot(chosen, tok_ref[...], preferred_element_type=F32)
        for s in range(experts):
            outs[s][...] = outgoing[s * capacity : (s + 1) * capacity].astype(BF16)
        gap = gap_ref[...]
        group = group_ref[...]
        info_ref[:, 0:1] = column(pos_first.astype(F32))
        info_ref[:, 1:2] = column(pos_second.astype(F32))
        info_ref[:, 2:3] = column(group * jax.nn.sigmoid(gap))
        info_ref[:, 3:4] = column(group * jax.nn.sigmoid(-gap))

    return pl.pallas_call(
        kernel,
        in_specs=[whole(VMEM)] * 4,
        out_specs=[whole(VMEM)] * (1 + experts),
        out_shape=[jax.ShapeDtypeStruct((rows, 4), F32)]
        + [jax.ShapeDtypeStruct((capacity, features), BF16)] * experts,
        compiler_params=GRANT,
        name="dispatch_rows",
    )(routes, group_weight, logit_gap, tokens)


def gate_up(pieces, chunks, capacity):
    n_tp, n_fs = len(pieces), len(chunks)
    ratio = n_fs // n_tp
    block, cols = chunks[0].shape[1:]
    slots = pieces[0].shape[0]

    def kernel(*refs):
        piece_refs = refs[:n_tp]
        chunk_refs = refs[n_tp : n_tp + n_fs]
        hidden_ref, gate_ref, up_ref, rows_ref, sems = refs[n_tp + n_fs :]
        own, lane = own_places()
        copies = []
        for s in range(n_fs):
            start = pl.multiple_of((own ^ s) * block, block)
            for w, out in enumerate((gate_ref, up_ref)):
                copy = pltpu.make_async_copy(
                    chunk_refs[s].at[w], out.at[0, pl.ds(start, block)], sems.at[s, w]
                )
                copy.start()
                copies.append(copy)
        for t in range(n_tp):
            for h in range(ratio):
                rows_ref[(lane ^ t) * ratio + h] = piece_refs[t][:, h * block : (h + 1) * block]
        gate_acc = jnp.zeros((slots, cols), F32)
        up_acc = jnp.zeros((slots, cols), F32)
        for s in range(n_fs):
            rows = rows_ref[own ^ s]
            gate_acc += jnp.dot(rows, chunk_refs[s][0], preferred_element_type=F32)
            up_acc += jnp.dot(rows, chunk_refs[s][1], preferred_element_type=F32)
        hidden_ref[...] = (gate_acc / (1.0 + jnp.exp(-gate_acc)) * up_acc).astype(BF16)
        for copy in copies:
            copy.wait()

    full = jax.ShapeDtypeStruct((1, n_fs * block, cols), BF16)
    return pl.pallas_call(
        kernel,
        in_specs=[whole(VMEM)] * (n_tp + n_fs),
        out_specs=[whole(VMEM), whole(ANY), whole(ANY)],
        out_shape=[jax.ShapeDtypeStruct((slots, cols), BF16), full, full],
        scratch_shapes=[VMEM((n_fs, slots, block), BF16), pltpu.SemaphoreType.DMA((n_fs, 2))],
        compiler_params=GRANT,
        name="gate_up",
    )(*pieces, *chunks)


def down(hiddens, chunks, n_fs, capacity):
    n_tp = len(hiddens)
    ratio = n_fs // n_tp
    slots, cols = hiddens[0].shape
    block = chunks[0].shape[1]

    def kernel(*refs):
        hidden_refs = refs[:n_tp]
        chunk_refs = refs[n_tp : n_tp + n_fs]
        back_refs = refs[n_tp + n_fs : n_tp + 2 * n_fs]
        piece_refs = refs[n_tp + 2 * n_fs : 2 * n_tp + 2 * n_fs]
        all_ref = refs[-1]
        own, lane = own_places()
        own_z, own_y = own // ratio, own % ratio
        for t in range(n_tp):
            all_ref[lane ^ t] = hidden_refs[t][...]
        for ky in range(ratio):
            total = jnp.zeros((slots, block), F32)
            for kz in range(n_tp):
                part = lax.dot_general(
                    all_ref[own_z ^ kz],
                    chunk_refs[kz * ratio + ky][0],
                    (((1,), (1,)), ((), ())),
                    preferred_element_type=F32,
                )
                total += part.astype(BF16).astype(F32)
            for s in range(n_fs):
                back_refs[s][own_y ^ ky] = total[s * capacity : (s + 1) * capacity].astype(BF16)
        for t in range(n_tp):
            for kz in range(n_tp):

                @pl.when((own_z ^ kz) == (lane ^ t))
                def _(t=t, kz=kz):
                    for ky in range(ratio):
                        piece_refs[t][own_y ^ ky] = chunk_refs[kz * ratio + ky][0]

    return pl.pallas_call(
        kernel,
        in_specs=[whole(VMEM)] * (n_tp + n_fs),
        out_specs=[whole(VMEM)] * (n_fs + n_tp),
        out_shape=[jax.ShapeDtypeStruct((ratio, capacity, block), BF16)] * n_fs
        + [jax.ShapeDtypeStruct((ratio, block, cols), BF16)] * n_tp,
        scratch_shapes=[VMEM((n_tp, slots, cols), BF16)],
        compiler_params=GRANT,
        name="down",
    )(*hiddens, *chunks)


def place(pieces):
    n_tp = len(pieces)
    ratio, block, cols = pieces[0].shape

    def kernel(*refs):
        out, sems = refs[n_tp:]
        _, lane = own_places()
        copies = []
        for t in range(n_tp):
            for h in range(ratio):
                start = pl.multiple_of(((lane ^ t) * ratio + h) * block, block)
                copy = pltpu.make_async_copy(
                    refs[t].at[h], out.at[0, pl.ds(start, block)], sems.at[t, h]
                )
                copy.start()
                copies.append(copy)
        for copy in copies:
            copy.wait()

    return pl.pallas_call(
        kernel,
        in_specs=[whole(VMEM)] * n_tp,
        out_specs=whole(ANY),
        out_shape=jax.ShapeDtypeStruct((1, n_tp * ratio * block, cols), BF16),
        scratch_shapes=[pltpu.SemaphoreType.DMA((n_tp, ratio))],
        compiler_params=GRANT,
        name="place",
    )(*pieces)


def combine(info, backs):
    n_fs = len(backs)
    ratio, capacity, block = backs[0].shape
    rows = info.shape[0]

    def kernel(info_ref, *refs):
        back_refs, out = refs[:n_fs], refs[n_fs]
        values = info_ref[...]
        both = jnp.concatenate([values[:, 0:1], values[:, 1:2]], axis=0).astype(jnp.int32)
        totals = [jnp.zeros((2 * rows, block), F32) for _ in range(ratio)]
        for s in range(n_fs):
            slots = lax.broadcasted_iota(jnp.int32, (2 * rows, capacity), 1) + s * capacity
            pick = (both == slots).astype(F32).astype(BF16)
            for h in range(ratio):
                totals[h] += jnp.dot(pick, back_refs[s][h], preferred_element_type=F32)
        for h in range(ratio):
            value = values[:, 2:3] * totals[h][:rows] + values[:, 3:4] * totals[h][rows:]
            out[:, h * block : (h + 1) * block] = value.astype(BF16)

    return pl.pallas_call(
        kernel,
        in_specs=[whole(VMEM)] * (1 + n_fs),
        out_specs=whole(VMEM),
        out_shape=jax.ShapeDtypeStruct((rows, ratio * block), BF16),
        compiler_params=GRANT,
        name="combine",
    )(info, *backs)


def exchange_body(
    n_fs,
    n_tp,
    tokens,
    norm_gain,
    gate_weight,
    up_weight,
    down_weight,
    route_ids,
    group_weight,
    logit_gap,
):
    experts = gate_weight.shape[0]
    tok_rows = tokens.shape[0]
    capacity = max(2, (3 * tok_rows + experts - 1) // experts)
    ratio = n_fs // n_tp
    far = [s ^ (n_fs - 1) for s in range(n_fs // 2)]
    near = [s ^ (n_fs - 1) for s in range(n_fs // 2, n_fs)]

    def swap_fs(value, s):
        return lax.ppermute(value, "fs", [(n, n ^ s) for n in range(n_fs)]) if s else value

    def swap_tp(value, s):
        return lax.ppermute(value, "tp", [(n, n ^ s) for n in range(n_tp)]) if s else value

    gain = norm_gain[None, :]

    def expert_of(s):
        return lambda own, lane: own ^ s

    far_cast = cast_chunks([expert_of(s) for s in far], gain, (gate_weight, up_weight))
    near_cast = cast_chunks([expert_of(s) for s in near], gain, (gate_weight, up_weight))
    local = dict(zip(far + near, list(far_cast) + list(near_cast)))
    chunks = {s: swap_fs(local[s], s) for s in far + near}

    info, *outgoing = dispatch_rows(
        route_ids.T, group_weight[None, :], logit_gap[None, :], tokens, experts, capacity
    )
    arrived = [swap_fs(outgoing[s], s) for s in range(n_fs)]
    slot_rows = jnp.concatenate(arrived, axis=0)
    pieces = [swap_tp(slot_rows, t) for t in range(n_tp)]

    moves = [(kz, ky) for kz in range(n_tp) for ky in range(ratio)]

    def expert_to(kz, ky):
        return lambda own, lane: (lane ^ kz) * ratio + ((own % ratio) ^ ky)

    down_cast = cast_chunks([expert_to(kz, ky) for kz, ky in moves], None, (down_weight,))
    down_chunks = []
    for (kz, ky), value in zip(moves, down_cast):
        pairs = [
            ((z * ratio + y) * n_tp + j, ((j ^ kz) * ratio + (y ^ ky)) * n_tp + z)
            for z in range(n_tp)
            for y in range(ratio)
            for j in range(n_tp)
        ]
        down_chunks.append(lax.ppermute(value, ("fs", "tp"), pairs))

    hidden, gate_out, up_out = gate_up(pieces, [chunks[s] for s in range(n_fs)], capacity)
    hiddens = [swap_tp(hidden, t) for t in range(n_tp)]
    results = down(hiddens, down_chunks, n_fs, capacity)
    backs, quarters = results[:n_fs], results[n_fs:]
    backs = [swap_fs(backs[s], s) for s in range(n_fs)]
    mixed = combine(info, backs)
    down_out = place([swap_tp(quarters[t], t) for t in range(n_tp)])
    return gate_out, up_out, down_out, mixed


def slot_tables(route_ids, experts, capacity):
    row_count = route_ids.shape[0]
    pair_count = 2 * row_count
    flat_ids = route_ids.reshape(pair_count)
    onehot = (flat_ids[:, None] == jnp.arange(experts, dtype=jnp.int32)[None, :]).astype(
        jnp.bfloat16
    )
    positions = jnp.arange(pair_count, dtype=jnp.int32)
    below_mask = (positions[:, None] > positions[None, :]).astype(jnp.bfloat16)
    before = jnp.dot(below_mask, onehot, preferred_element_type=jnp.float32)
    ranked = jnp.sum(before * onehot.astype(jnp.float32), axis=1).astype(jnp.int32)
    return (flat_ids * capacity + ranked).reshape(row_count, 2)


def first_products(slot_rows, gate_cols, up_cols):
    shard_cols = lax.all_gather(slot_rows, "tp", axis=1, tiled=True)
    return (
        jnp.dot(shard_cols, gate_cols, preferred_element_type=jnp.float32),
        jnp.dot(shard_cols, up_cols, preferred_element_type=jnp.float32),
    )


def body(
    tokens, norm_gain, gate_weight, up_weight, down_weight, route_ids, group_weight, logit_gap
):
    experts = gate_weight.shape[0]
    tok_rows = tokens.shape[0]
    capacity = max(2, (3 * tok_rows + experts - 1) // experts)
    folded = norm_gain[None, :, None]
    gate_local = (gate_weight * folded).astype(jnp.bfloat16)
    up_local = (up_weight * folded).astype(jnp.bfloat16)
    down_local = down_weight.astype(jnp.bfloat16)
    slot_ids = slot_tables(route_ids, experts, capacity)
    slot_range = jnp.arange(experts * capacity, dtype=jnp.int32)
    matches = (slot_ids[None, :, :] == slot_range[:, None, None]).astype(jnp.int32)
    dispatch = jnp.sum(matches, axis=2).astype(jnp.bfloat16)
    outgoing = jnp.dot(dispatch, tokens, preferred_element_type=jnp.float32).astype(jnp.bfloat16)
    outgoing = outgoing.reshape(experts, capacity, tokens.shape[1])
    arrived = lax.all_to_all(outgoing, "fs", split_axis=0, concat_axis=0, tiled=True)
    slot_rows = arrived.reshape(experts * capacity, tokens.shape[1])
    gate_out, up_out, down_out = (
        lax.all_to_all(gate_local, "fs", split_axis=0, concat_axis=1, tiled=True),
        lax.all_to_all(up_local, "fs", split_axis=0, concat_axis=1, tiled=True),
        lax.all_to_all(down_local, "fs", split_axis=0, concat_axis=1, tiled=True),
    )
    gate_acc, up_acc = first_products(slot_rows, gate_out[0], up_out[0])
    hidden = (jax.nn.silu(gate_acc) * up_acc).astype(jnp.bfloat16)
    partial_value = lax.dot_general(
        hidden, down_out[0], (((1,), (1,)), ((), ())), preferred_element_type=jnp.float32
    )
    summed = lax.psum_scatter(
        partial_value.astype(jnp.bfloat16), "tp", scatter_dimension=1, tiled=True
    )
    returned = lax.all_to_all(
        summed.reshape(experts, capacity, summed.shape[1]),
        "fs",
        split_axis=0,
        concat_axis=0,
        tiled=True,
    )
    back_rows = returned.reshape(experts * capacity, summed.shape[1])
    pick_first = (slot_ids[:, 0:1] == slot_range[None, :]).astype(jnp.bfloat16)
    pick_second = (slot_ids[:, 1:2] == slot_range[None, :]).astype(jnp.bfloat16)
    first_vals = jnp.dot(pick_first, back_rows, preferred_element_type=jnp.float32)
    second_vals = jnp.dot(pick_second, back_rows, preferred_element_type=jnp.float32)
    first_weight = group_weight * jax.nn.sigmoid(logit_gap)
    second_weight = group_weight * jax.nn.sigmoid(-logit_gap)
    mixed = (first_weight[:, None] * first_vals + second_weight[:, None] * second_vals).astype(
        jnp.bfloat16
    )
    return (gate_out, up_out, down_out, mixed)


def solution(mesh):
    n_fs, n_tp = mesh.shape["fs"], mesh.shape["tp"]
    small = n_fs <= 16 and n_fs % n_tp == 0 and n_fs & (n_fs - 1) == 0
    return jax.shard_map(
        functools.partial(exchange_body, n_fs, n_tp) if small else body,
        mesh=mesh,
        in_specs=(
            P("fs", "tp"),
            P("fs"),
            P(None, "fs", "tp"),
            P(None, "fs", "tp"),
            P(None, "fs", "tp"),
            P("fs", None),
            P("fs"),
            P("fs"),
        ),
        out_specs=(P("fs", None, "tp"), P("fs", None, "tp"), P("fs", None, "tp"), P("fs", "tp")),
        check_vma=False,
    )
```

```python
import jax
import jax.numpy as jnp
from jax import lax
from jax.experimental import pallas as pl
from jax.experimental.pallas import tpu as pltpu
from jax.sharding import PartitionSpec as P


BF16 = jnp.bfloat16
F32 = jnp.float32


GRANT = pltpu.CompilerParams(vmem_limit_bytes=8 * 1024 * 1024)
VMEM = pltpu.VMEM
ANY = pl.ANY


def whole(space):
    return pl.BlockSpec(memory_space=space)


def column(row):
    n = row.shape[1]
    same = lax.broadcasted_iota(jnp.int32, (n, n), 0) == lax.broadcasted_iota(jnp.int32, (n, n), 1)
    return jnp.sum(jnp.where(same, row, 0.0), axis=1, keepdims=True)


def own_places():
    return lax.axis_index("fs").astype(jnp.int32), lax.axis_index("tp").astype(jnp.int32)


def cast_chunks(picks, gain, weights):
    count, stack = len(picks), len(weights)
    rows, cols = weights[0].shape[1:]

    def kernel(gain_ref, *refs):
        sources = refs[:stack]
        targets = refs[stack:]
        own, _ = own_places()
        factor = column(gain_ref[...])
        for n in range(count):
            for w in range(stack):
                targets[n][w] = (sources[w][own ^ picks[n]] * factor).astype(BF16)

    return pl.pallas_call(
        kernel,
        in_specs=[whole(VMEM)] * (1 + stack),
        out_specs=[whole(VMEM)] * count,
        out_shape=[jax.ShapeDtypeStruct((stack, rows, cols), BF16)] * count,
        compiler_params=GRANT,
        name="cast_chunks",
    )(gain, *weights)


def cast_rows(weight, n_tp):
    experts, rows, cols = weight.shape
    part = rows // n_tp

    def kernel(source, *targets):
        own, lane = own_places()
        for t in range(n_tp):
            start = pl.multiple_of((lane ^ t) * part, part)
            for s in range(experts):
                targets[t][s] = source[own ^ s, pl.ds(start, part), :].astype(BF16)

    return pl.pallas_call(
        kernel,
        in_specs=[whole(VMEM)],
        out_specs=[whole(VMEM)] * n_tp,
        out_shape=[jax.ShapeDtypeStruct((experts, part, cols), BF16)] * n_tp,
        compiler_params=GRANT,
        name="cast_rows",
    )(weight)


def regroup(parts):
    inner, outer = len(parts), parts[0].shape[0]

    def kernel(*refs):
        for s in range(outer):
            for t in range(inner):
                refs[inner + s][t] = refs[t][s]

    return pl.pallas_call(
        kernel,
        in_specs=[whole(VMEM)] * inner,
        out_specs=[whole(VMEM)] * outer,
        out_shape=[jax.ShapeDtypeStruct((inner,) + parts[0].shape[1:], parts[0].dtype)] * outer,
        compiler_params=GRANT,
        name="regroup",
    )(*parts)


def dispatch_rows(routes, group_weight, logit_gap, tokens, experts, capacity):
    rows, features = tokens.shape

    def kernel(route_ref, group_ref, gap_ref, tok_ref, info_ref, out_ref):
        first = route_ref[0:1, :]
        second = route_ref[1:2, :]
        names = lax.broadcasted_iota(jnp.int32, (experts, rows), 0)
        hit_first = (names == first).astype(F32)
        hit_second = (names == second).astype(F32)
        above = lax.broadcasted_iota(jnp.int32, (rows, rows), 0) < lax.broadcasted_iota(
            jnp.int32, (rows, rows), 1
        )
        before = jnp.dot(
            (hit_first + hit_second).astype(BF16),
            above.astype(F32).astype(BF16),
            preferred_element_type=F32,
        )
        rank_first = jnp.sum(before * hit_first, axis=0, keepdims=True)
        rank_second = jnp.sum(before * hit_second, axis=0, keepdims=True)
        pos_first = first * capacity + rank_first.astype(jnp.int32)
        pos_second = second * capacity + rank_second.astype(jnp.int32)
        slots = lax.broadcasted_iota(jnp.int32, (experts * capacity, rows), 0)
        chosen = ((pos_first == slots) | (pos_second == slots)).astype(F32).astype(BF16)
        outgoing = jnp.dot(chosen, tok_ref[...], preferred_element_type=F32)
        for s in range(experts):
            out_ref[s] = outgoing[s * capacity : (s + 1) * capacity].astype(BF16)
        gap = gap_ref[...]
        group = group_ref[...]
        info_ref[:, 0:1] = column(pos_first.astype(F32))
        info_ref[:, 1:2] = column(pos_second.astype(F32))
        info_ref[:, 2:3] = column(group * jax.nn.sigmoid(gap))
        info_ref[:, 3:4] = column(group * jax.nn.sigmoid(-gap))

    return pl.pallas_call(
        kernel,
        in_specs=[whole(VMEM)] * 4,
        out_specs=[whole(VMEM)] * 2,
        out_shape=[
            jax.ShapeDtypeStruct((rows, 4), F32),
            jax.ShapeDtypeStruct((experts, capacity, features), BF16),
        ],
        compiler_params=GRANT,
        name="dispatch_rows",
    )(routes, group_weight, logit_gap, tokens)


def gate_up(pieces, chunks):
    n_tp, n_fs = len(pieces), len(chunks)
    ratio = n_fs // n_tp
    block, cols = chunks[0].shape[1:]
    slots = pieces[0].shape[0]

    def kernel(*refs):
        piece_refs = refs[:n_tp]
        chunk_refs = refs[n_tp : n_tp + n_fs]
        hidden_ref, gate_ref, up_ref, rows_ref, sems = refs[n_tp + n_fs :]
        own, lane = own_places()
        copies = []
        for s in range(n_fs):
            start = pl.multiple_of((own ^ s) * block, block)
            for w, out in enumerate((gate_ref, up_ref)):
                copy = pltpu.make_async_copy(
                    chunk_refs[s].at[w], out.at[0, pl.ds(start, block)], sems.at[s, w]
                )
                copy.start()
                copies.append(copy)
        for t in range(n_tp):
            for h in range(ratio):
                rows_ref[(lane ^ t) * ratio + h] = piece_refs[t][:, h * block : (h + 1) * block]
        gate_acc = jnp.zeros((slots, cols), F32)
        up_acc = jnp.zeros((slots, cols), F32)
        for s in range(n_fs):
            rows = rows_ref[own ^ s]
            gate_acc += jnp.dot(rows, chunk_refs[s][0], preferred_element_type=F32)
            up_acc += jnp.dot(rows, chunk_refs[s][1], preferred_element_type=F32)
        hidden_ref[...] = (gate_acc / (1.0 + jnp.exp(-gate_acc)) * up_acc).astype(BF16)
        for copy in copies:
            copy.wait()

    full = jax.ShapeDtypeStruct((1, n_fs * block, cols), BF16)
    return pl.pallas_call(
        kernel,
        in_specs=[whole(VMEM)] * (n_tp + n_fs),
        out_specs=[whole(VMEM), whole(ANY), whole(ANY)],
        out_shape=[jax.ShapeDtypeStruct((slots, cols), BF16), full, full],
        scratch_shapes=[VMEM((n_fs, slots, block), BF16), pltpu.SemaphoreType.DMA((n_fs, 2))],
        compiler_params=GRANT,
        name="gate_up",
    )(*pieces, *chunks)


def down(hiddens, chunks, capacity):
    n_tp, n_fs = len(hiddens), len(chunks)
    ratio = n_fs // n_tp
    slots, cols = hiddens[0].shape
    part = chunks[0].shape[1]

    def kernel(*refs):
        hidden_refs = refs[:n_tp]
        chunk_refs = refs[n_tp : n_tp + n_fs]
        out_ref, all_ref = refs[n_tp + n_fs :]
        own, _ = own_places()
        for s in range(n_fs):
            for t in range(n_tp):
                all_ref[t, s * part : (s + 1) * part] = chunk_refs[s][t]
        total = jnp.zeros((slots, n_fs * part), F32)
        for t in range(n_tp):
            product = lax.dot_general(
                hidden_refs[t][...],
                all_ref[t],
                (((1,), (1,)), ((), ())),
                preferred_element_type=F32,
            )
            total += product.astype(BF16).astype(F32)
        wide = ratio * part
        for m in range(n_tp):
            for b in range(n_fs):
                out_ref[b * n_tp + ((own // ratio) ^ m)] = total[
                    b * capacity : (b + 1) * capacity, m * wide : (m + 1) * wide
                ].astype(BF16)

    return pl.pallas_call(
        kernel,
        in_specs=[whole(VMEM)] * (n_tp + n_fs),
        out_specs=whole(VMEM),
        out_shape=jax.ShapeDtypeStruct((n_fs * n_tp, capacity, ratio * part), BF16),
        scratch_shapes=[VMEM((n_tp, n_fs * part, cols), BF16)],
        compiler_params=GRANT,
        name="down",
    )(*hiddens, *chunks)


def finish(info, back, pieces):
    n_tp = len(pieces)
    n_fs, part, cols = pieces[0].shape
    capacity, wide = back.shape[1:]
    ratio = wide // part
    rows = info.shape[0]

    def kernel(info_ref, back_ref, *refs):
        piece_refs = refs[:n_tp]
        out, down_ref, sems = refs[n_tp:]
        own, lane = own_places()
        copies = []
        for t in range(n_tp):
            for s in range(n_fs):
                start = pl.multiple_of(((own ^ s) * n_tp + (lane ^ t)) * part, part)
                copy = pltpu.make_async_copy(
                    piece_refs[t].at[s], down_ref.at[0, pl.ds(start, part)], sems.at[t, s]
                )
                copy.start()
                copies.append(copy)
        values = info_ref[...]
        both = jnp.concatenate([values[:, 0:1], values[:, 1:2]], axis=0).astype(jnp.int32)
        picks = []
        for e in range(n_fs):
            slots = lax.broadcasted_iota(jnp.int32, (2 * rows, capacity), 1) + e * capacity
            picks.append((both == slots).astype(F32).astype(BF16))
        for j in range(n_tp):
            halves = [jnp.zeros((2 * rows, wide), F32) for _ in range(ratio)]
            for e in range(n_fs):
                halves[e % ratio] += jnp.dot(
                    picks[e], back_ref[e * n_tp + j], preferred_element_type=F32
                )
            for y in range(ratio):
                total = sum(
                    halves[k][:, (y ^ k) * part : ((y ^ k) + 1) * part] for k in range(ratio)
                )
                value = values[:, 2:3] * total[:rows] + values[:, 3:4] * total[rows:]
                at = (y * n_tp + j) * part
                out[:, at : at + part] = value.astype(BF16)
        for copy in copies:
            copy.wait()

    return pl.pallas_call(
        kernel,
        in_specs=[whole(VMEM)] * (2 + n_tp),
        out_specs=[whole(VMEM), whole(ANY)],
        out_shape=[
            jax.ShapeDtypeStruct((rows, n_tp * wide), BF16),
            jax.ShapeDtypeStruct((1, n_fs * n_tp * part, cols), BF16),
        ],
        scratch_shapes=[pltpu.SemaphoreType.DMA((n_tp, n_fs))],
        compiler_params=GRANT,
        name="finish",
    )(info, back, *pieces)


def exchange_body(
    n_fs,
    n_tp,
    tokens,
    norm_gain,
    gate_weight,
    up_weight,
    down_weight,
    route_ids,
    group_weight,
    logit_gap,
):
    experts = gate_weight.shape[0]
    tok_rows = tokens.shape[0]
    capacity = max(2, (3 * tok_rows + experts - 1) // experts)
    far = [s ^ (n_fs - 1) for s in range(n_fs // 2)]
    near = [s ^ (n_fs - 1) for s in range(n_fs // 2, n_fs)]

    def swap_fs(value, s):
        if s == 0:
            return value
        return lax.ppermute(value, "fs", [(n, n ^ s) for n in range(n_fs)])

    def swap_tp(value, s):
        if s == 0:
            return value
        return lax.ppermute(value, "tp", [(n, n ^ s) for n in range(n_tp)])

    gain = norm_gain[None, :]
    far_cast = cast_chunks(far, gain, (gate_weight, up_weight))
    near_cast = cast_chunks(near, gain, (gate_weight, up_weight))
    local = dict(zip(far + near, list(far_cast) + list(near_cast)))
    chunks = [swap_fs(local[s], s) for s in range(n_fs)]

    info, outgoing = dispatch_rows(
        route_ids.T, group_weight[None, :], logit_gap[None, :], tokens, experts, capacity
    )
    arrived = lax.all_to_all(outgoing, "fs", split_axis=0, concat_axis=0, tiled=True)
    slot_rows = arrived.reshape(n_fs * capacity, tokens.shape[1])
    pieces = [swap_tp(slot_rows, t) for t in range(n_tp)]

    down_parts = cast_rows(down_weight, n_tp)
    down_parts = [swap_tp(down_parts[t], t) for t in range(n_tp)]
    down_local = regroup(down_parts)
    down_chunks = [swap_fs(down_local[s], s) for s in range(n_fs)]
    quarters = regroup(down_chunks)
    quarters = [swap_tp(quarters[t], t) for t in range(n_tp)]

    hidden, gate_out, up_out = gate_up(pieces, chunks)
    hiddens = [swap_tp(hidden, t) for t in range(n_tp)]
    rows = down(hiddens, down_chunks, capacity)
    back = lax.all_to_all(rows, ("fs", "tp"), split_axis=0, concat_axis=0, tiled=True)
    mixed, down_out = finish(info, back, quarters)
    return gate_out, up_out, down_out, mixed


def slot_tables(route_ids, experts, capacity):
    row_count = route_ids.shape[0]
    pair_count = 2 * row_count
    flat_ids = route_ids.reshape(pair_count)
    onehot = (flat_ids[:, None] == jnp.arange(experts, dtype=jnp.int32)[None, :]).astype(
        jnp.bfloat16
    )
    positions = jnp.arange(pair_count, dtype=jnp.int32)
    below_mask = (positions[:, None] > positions[None, :]).astype(jnp.bfloat16)
    before = jnp.dot(below_mask, onehot, preferred_element_type=jnp.float32)
    ranked = jnp.sum(before * onehot.astype(jnp.float32), axis=1).astype(jnp.int32)
    return (flat_ids * capacity + ranked).reshape(row_count, 2)


def first_products(slot_rows, gate_cols, up_cols):
    shard_cols = lax.all_gather(slot_rows, "tp", axis=1, tiled=True)
    return (
        jnp.dot(shard_cols, gate_cols, preferred_element_type=jnp.float32),
        jnp.dot(shard_cols, up_cols, preferred_element_type=jnp.float32),
    )


def body(
    tokens, norm_gain, gate_weight, up_weight, down_weight, route_ids, group_weight, logit_gap
):
    experts = gate_weight.shape[0]
    tok_rows = tokens.shape[0]
    capacity = max(2, (3 * tok_rows + experts - 1) // experts)
    folded = norm_gain[None, :, None]
    gate_local = (gate_weight * folded).astype(jnp.bfloat16)
    up_local = (up_weight * folded).astype(jnp.bfloat16)
    down_local = down_weight.astype(jnp.bfloat16)
    slot_ids = slot_tables(route_ids, experts, capacity)
    slot_range = jnp.arange(experts * capacity, dtype=jnp.int32)
    matches = (slot_ids[None, :, :] == slot_range[:, None, None]).astype(jnp.int32)
    dispatch = jnp.sum(matches, axis=2).astype(jnp.bfloat16)
    outgoing = jnp.dot(dispatch, tokens, preferred_element_type=jnp.float32).astype(jnp.bfloat16)
    outgoing = outgoing.reshape(experts, capacity, tokens.shape[1])
    arrived = lax.all_to_all(outgoing, "fs", split_axis=0, concat_axis=0, tiled=True)
    slot_rows = arrived.reshape(experts * capacity, tokens.shape[1])
    gate_out, up_out, down_out = (
        lax.all_to_all(gate_local, "fs", split_axis=0, concat_axis=1, tiled=True),
        lax.all_to_all(up_local, "fs", split_axis=0, concat_axis=1, tiled=True),
        lax.all_to_all(down_local, "fs", split_axis=0, concat_axis=1, tiled=True),
    )
    gate_acc, up_acc = first_products(slot_rows, gate_out[0], up_out[0])
    hidden = (jax.nn.silu(gate_acc) * up_acc).astype(jnp.bfloat16)
    partial_value = lax.dot_general(
        hidden, down_out[0], (((1,), (1,)), ((), ())), preferred_element_type=jnp.float32
    )
    summed = lax.psum_scatter(
        partial_value.astype(jnp.bfloat16), "tp", scatter_dimension=1, tiled=True
    )
    returned = lax.all_to_all(
        summed.reshape(experts, capacity, summed.shape[1]),
        "fs",
        split_axis=0,
        concat_axis=0,
        tiled=True,
    )
    back_rows = returned.reshape(experts * capacity, summed.shape[1])
    pick_first = (slot_ids[:, 0:1] == slot_range[None, :]).astype(jnp.bfloat16)
    pick_second = (slot_ids[:, 1:2] == slot_range[None, :]).astype(jnp.bfloat16)
    first_vals = jnp.dot(pick_first, back_rows, preferred_element_type=jnp.float32)
    second_vals = jnp.dot(pick_second, back_rows, preferred_element_type=jnp.float32)
    first_weight = group_weight * jax.nn.sigmoid(logit_gap)
    second_weight = group_weight * jax.nn.sigmoid(-logit_gap)
    mixed = (first_weight[:, None] * first_vals + second_weight[:, None] * second_vals).astype(
        jnp.bfloat16
    )
    return (gate_out, up_out, down_out, mixed)


def solution(mesh):
    n_fs, n_tp = mesh.shape["fs"], mesh.shape["tp"]
    small = n_fs <= 16 and n_fs % n_tp == 0 and n_fs & (n_fs - 1) == 0

    def step(*args):
        if not small:
            return body(*args)
        return exchange_body(n_fs, n_tp, *args)

    return jax.shard_map(
        step,
        mesh=mesh,
        in_specs=(
            P("fs", "tp"),
            P("fs"),
            P(None, "fs", "tp"),
            P(None, "fs", "tp"),
            P(None, "fs", "tp"),
            P("fs", None),
            P("fs"),
            P("fs"),
        ),
        out_specs=(P("fs", None, "tp"), P("fs", None, "tp"), P("fs", None, "tp"), P("fs", "tp")),
        check_vma=False,
    )
```

```python
import jax
import jax.numpy as jnp
from jax import lax
from jax.experimental import pallas as pl
from jax.experimental.pallas import tpu as pltpu
from jax.sharding import PartitionSpec as P


BF16 = jnp.bfloat16
F32 = jnp.float32


GRANT = pltpu.CompilerParams(vmem_limit_bytes=8 * 1024 * 1024)
VMEM = pltpu.VMEM
ANY = pl.ANY


def whole(space):
    return pl.BlockSpec(memory_space=space)


def column(row):
    n = row.shape[1]
    same = lax.broadcasted_iota(jnp.int32, (n, n), 0) == lax.broadcasted_iota(jnp.int32, (n, n), 1)
    return jnp.sum(jnp.where(same, row, 0.0), axis=1, keepdims=True)


def own_places():
    return lax.axis_index("fs").astype(jnp.int32), lax.axis_index("tp").astype(jnp.int32)


def put_rows(target, base, rows):
    capacity, features = rows.shape
    cols = target.shape[1]
    for c in range(features // cols):
        at = base + c * capacity
        target[at : at + capacity, :] = rows[:, c * cols : (c + 1) * cols]


def fetch(pairs, sems):
    copies = []
    for n, (source, target) in enumerate(pairs):
        copy = pltpu.make_async_copy(source, target, sems.at[n])
        copy.start()
        copies.append(copy)
    return copies


def start_first(
    steps, later, routes, group_weight, logit_gap, tokens, gain, weights, capacity, ratio
):
    tok_rows, features = tokens.shape
    experts, block, cols = weights[0].shape
    stack, count = len(weights), len(steps)
    lanes = features // cols
    height = stack * block + lanes * capacity
    small = (routes, group_weight, logit_gap, tokens, gain)

    def kernel(*refs):
        small_in = refs[: len(small)]
        sources = refs[len(small) : len(small) + stack]
        at = len(small) + stack
        info_ref, later_ref = refs[at : at + 2]
        targets = refs[at + 2 : at + 2 + count]
        small_refs = refs[at + 2 + count : at + 2 + count + len(small)]
        buffer, small_sems, sems = refs[at + 2 + count + len(small) :]
        route_ref, group_ref, gap_ref, tok_ref, gain_ref = small_refs
        own, _ = own_places()
        small_copies = fetch(list(zip(small_in, small_refs)), small_sems)
        order = [(n, w) for n in range(count) for w in range(stack)]
        copies = fetch(
            [(sources[w].at[own ^ steps[n]], buffer.at[n, w]) for n, w in order], sems
        )
        for copy in small_copies:
            copy.wait()
        first = route_ref[0:1, :]
        second = route_ref[1:2, :]
        names = lax.broadcasted_iota(jnp.int32, (experts, tok_rows), 0)
        hit_first = (names == first).astype(F32)
        hit_second = (names == second).astype(F32)
        shape = (tok_rows, tok_rows)
        above = lax.broadcasted_iota(jnp.int32, shape, 0) < lax.broadcasted_iota(jnp.int32, shape, 1)
        before = jnp.dot(
            (hit_first + hit_second).astype(BF16),
            above.astype(F32).astype(BF16),
            preferred_element_type=F32,
        )
        rank_first = jnp.sum(before * hit_first, axis=0, keepdims=True).astype(jnp.int32)
        rank_second = jnp.sum(before * hit_second, axis=0, keepdims=True).astype(jnp.int32)
        slots = lax.broadcasted_iota(jnp.int32, (experts * capacity, tok_rows), 0)
        there_first = (first ^ own) * capacity + rank_first
        there_second = (second ^ own) * capacity + rank_second
        chosen = ((there_first == slots) | (there_second == slots)).astype(F32).astype(BF16)
        outgoing = jnp.dot(chosen, tok_ref[...], preferred_element_type=F32).astype(BF16)
        for n, s in enumerate(steps):
            put_rows(targets[n], stack * block, outgoing[s * capacity : (s + 1) * capacity])
        for n, s in enumerate(later):
            put_rows(later_ref.at[n], 0, outgoing[s * capacity : (s + 1) * capacity])
        gap = gap_ref[...]
        group = group_ref[...]
        info_ref[:, 0:1] = column(group * jax.nn.sigmoid(gap))
        info_ref[:, 1:2] = column(group * jax.nn.sigmoid(-gap))
        for k in range(ratio):
            for c, (name, rank) in enumerate(((first, rank_first), (second, rank_second))):
                place = (name // ratio) * capacity + rank
                place = jnp.where(name % ratio == k, place, -1)
                info_ref[:, 2 + 2 * k + c : 3 + 2 * k + c] = column(place.astype(F32))
        factor = column(gain_ref[...])
        for (n, w), copy in zip(order, copies):
            copy.wait()
            targets[n][w * block : (w + 1) * block, :] = (buffer[n, w] * factor).astype(BF16)

    return pl.pallas_call(
        kernel,
        in_specs=[whole(ANY)] * (len(small) + stack),
        out_specs=[whole(VMEM)] * (2 + count),
        out_shape=[
            jax.ShapeDtypeStruct((tok_rows, 2 + 2 * ratio), F32),
            jax.ShapeDtypeStruct((len(later), lanes * capacity, cols), BF16),
        ]
        + [jax.ShapeDtypeStruct((height, cols), BF16)] * count,
        scratch_shapes=[VMEM(value.shape, value.dtype) for value in small]
        + [
            VMEM((count, stack, block, cols), F32),
            pltpu.SemaphoreType.DMA((len(small),)),
            pltpu.SemaphoreType.DMA((count * stack,)),
        ],
        compiler_params=GRANT,
        name="start_first",
    )(*small, *weights)


def start_later(steps, later_rows, gain, weights):
    stack, count = len(weights), len(steps)
    block, cols = weights[0].shape[1:]
    tail = later_rows.shape[1]

    def kernel(rows_ref, gain_ref, *refs):
        sources = refs[:stack]
        targets = refs[stack : stack + count]
        buffer, sems = refs[stack + count :]
        own, _ = own_places()
        order = [(n, w) for n in range(count) for w in range(stack)]
        copies = fetch(
            [(sources[w].at[own ^ steps[n]], buffer.at[n, w]) for n, w in order], sems
        )
        factor = column(gain_ref[...])
        for n in range(count):
            targets[n][stack * block :, :] = rows_ref[n]
        for (n, w), copy in zip(order, copies):
            copy.wait()
            targets[n][w * block : (w + 1) * block, :] = (buffer[n, w] * factor).astype(BF16)

    return pl.pallas_call(
        kernel,
        in_specs=[whole(VMEM)] * 2 + [whole(ANY)] * stack,
        out_specs=[whole(VMEM)] * count,
        out_shape=[jax.ShapeDtypeStruct((stack * block + tail, cols), BF16)] * count,
        scratch_shapes=[
            VMEM((count, stack, block, cols), F32),
            pltpu.SemaphoreType.DMA((count * stack,)),
        ],
        compiler_params=GRANT,
        name="start_later",
    )(later_rows, gain, *weights)


def slot_rows_of(chunks, base, capacity):
    count = len(chunks)
    height, cols = chunks[0].shape
    lanes = (height - base) // capacity

    def kernel(*refs):
        out = refs[count]
        for n in range(count):
            for c in range(lanes):
                at = base + c * capacity
                out[n * capacity : (n + 1) * capacity, c * cols : (c + 1) * cols] = refs[n][
                    at : at + capacity, :
                ]

    return pl.pallas_call(
        kernel,
        in_specs=[whole(VMEM)] * count,
        out_specs=whole(VMEM),
        out_shape=jax.ShapeDtypeStruct((count * capacity, lanes * cols), BF16),
        compiler_params=GRANT,
        name="slot_rows",
    )(*chunks)


def cast_rows(weight, n_tp):
    experts, rows, cols = weight.shape
    part = rows // n_tp

    def kernel(source, *refs):
        targets = refs[:n_tp]
        buffer, sems = refs[n_tp:]
        own, lane = own_places()
        copies = fetch([(source.at[own ^ s], buffer.at[s]) for s in range(experts)], sems)
        for s, copy in enumerate(copies):
            copy.wait()
            for t in range(n_tp):
                start = pl.multiple_of((lane ^ t) * part, part)
                targets[t][s] = buffer[s, pl.ds(start, part), :].astype(BF16)

    return pl.pallas_call(
        kernel,
        in_specs=[whole(ANY)],
        out_specs=[whole(VMEM)] * n_tp,
        out_shape=[jax.ShapeDtypeStruct((experts, part, cols), BF16)] * n_tp,
        scratch_shapes=[
            VMEM((experts, rows, cols), F32),
            pltpu.SemaphoreType.DMA((experts,)),
        ],
        compiler_params=GRANT,
        name="cast_rows",
    )(weight)


def regroup(parts):
    inner, outer = len(parts), parts[0].shape[0]

    def kernel(*refs):
        for s in range(outer):
            for t in range(inner):
                refs[inner + s][t] = refs[t][s]

    return pl.pallas_call(
        kernel,
        in_specs=[whole(VMEM)] * inner,
        out_specs=[whole(VMEM)] * outer,
        out_shape=[jax.ShapeDtypeStruct((inner,) + parts[0].shape[1:], parts[0].dtype)] * outer,
        compiler_params=GRANT,
        name="regroup",
    )(*parts)


def gate_up(parts, chunks, block):
    n_fs, n_tp = len(chunks), len(parts[0])
    ratio = n_fs // n_tp
    cols = chunks[0].shape[1]
    counts = [batch[0].shape[0] for batch in parts]
    slots = sum(counts)
    flat = [piece for batch in parts for piece in batch]

    def kernel(*refs):
        piece_refs = refs[: len(flat)]
        chunk_refs = refs[len(flat) : len(flat) + n_fs]
        hidden_ref, rows_ref = refs[len(flat) + n_fs :]
        own, lane = own_places()
        at = 0
        for k, count in enumerate(counts):
            for t in range(n_tp):
                for h in range(ratio):
                    rows_ref[(lane ^ t) * ratio + h, at : at + count] = piece_refs[k * n_tp + t][
                        :, h * block : (h + 1) * block
                    ]
            at += count
        gate_acc = jnp.zeros((slots, cols), F32)
        up_acc = jnp.zeros((slots, cols), F32)
        for s in range(n_fs):
            rows = rows_ref[own ^ s]
            gate_acc += jnp.dot(rows, chunk_refs[s][:block], preferred_element_type=F32)
            up_acc += jnp.dot(rows, chunk_refs[s][block : 2 * block], preferred_element_type=F32)
        hidden_ref[...] = (gate_acc / (1.0 + jnp.exp(-gate_acc)) * up_acc).astype(BF16)

    return pl.pallas_call(
        kernel,
        in_specs=[whole(VMEM)] * (len(flat) + n_fs),
        out_specs=whole(VMEM),
        out_shape=jax.ShapeDtypeStruct((slots, cols), BF16),
        scratch_shapes=[VMEM((n_fs, slots, block), BF16)],
        compiler_params=GRANT,
        name="gate_up",
    )(*flat, *chunks)


def gather_blocks(batch, pieces, own, lane, block_ref, down_ref, sems):
    n_tp = len(pieces)
    part = pieces[0].shape[1]
    block = n_tp * part
    copies = []
    for n, s in enumerate(batch):
        for t in range(n_tp):
            at = pl.multiple_of((lane ^ t) * part, part)
            block_ref[n, pl.ds(at, part), :] = pieces[t][n]
        start = pl.multiple_of((own ^ s) * block, block)
        copy = pltpu.make_async_copy(
            block_ref.at[n], down_ref.at[0, pl.ds(start, block)], sems.at[n]
        )
        copy.start()
        copies.append(copy)
    return copies


def store(chunks, block, batch, pieces):
    n_fs, n_tp = len(chunks), len(pieces)
    cols = chunks[0].shape[1]

    def kernel(*refs):
        piece_refs = refs[n_fs : n_fs + n_tp]
        outs = refs[n_fs + n_tp : n_fs + n_tp + 3]
        block_ref, sems, down_sems = refs[n_fs + n_tp + 3 :]
        own, lane = own_places()
        copies = gather_blocks(batch, piece_refs, own, lane, block_ref, outs[2], down_sems)
        for s in range(n_fs):
            start = pl.multiple_of((own ^ s) * block, block)
            for w in range(2):
                copy = pltpu.make_async_copy(
                    refs[s].at[pl.ds(w * block, block)],
                    outs[w].at[0, pl.ds(start, block)],
                    sems.at[s, w],
                )
                copy.start()
                copies.append(copy)
        for copy in copies:
            copy.wait()

    full = jax.ShapeDtypeStruct((1, n_fs * block, cols), BF16)
    return pl.pallas_call(
        kernel,
        in_specs=[whole(VMEM)] * (n_fs + n_tp),
        out_specs=[whole(ANY)] * 3,
        out_shape=[full] * 3,
        scratch_shapes=[
            VMEM((len(batch), block, cols), BF16),
            pltpu.SemaphoreType.DMA((n_fs, 2)),
            pltpu.SemaphoreType.DMA((len(batch),)),
        ],
        compiler_params=GRANT,
        name="store",
    )(*chunks, *pieces)


def down(row_order, hiddens, chunks, capacity):
    n_tp, n_fs = len(hiddens), len(chunks)
    ratio = n_fs // n_tp
    slots, cols = hiddens[0].shape
    part = chunks[0].shape[1]

    def kernel(*refs):
        hidden_refs = refs[:n_tp]
        chunk_refs = refs[n_tp : n_tp + n_fs]
        out_ref, hidden_ref, all_ref = refs[n_tp + n_fs :]
        own, _ = own_places()
        for t in range(n_tp):
            hidden_ref[:, t * cols : (t + 1) * cols] = hidden_refs[t][...]
            for s in range(n_fs):
                all_ref[s * part : (s + 1) * part, t * cols : (t + 1) * cols] = chunk_refs[s][t]
        total = lax.dot_general(
            hidden_ref[...], all_ref[...], (((1,), (1,)), ((), ())), preferred_element_type=F32
        )
        wide = ratio * part
        for m in range(n_tp):
            for k, s in enumerate(row_order):
                out_ref[(own ^ s) * n_tp + ((own // ratio) ^ m)] = total[
                    k * capacity : (k + 1) * capacity, m * wide : (m + 1) * wide
                ].astype(BF16)

    return pl.pallas_call(
        kernel,
        in_specs=[whole(VMEM)] * (n_tp + n_fs),
        out_specs=whole(VMEM),
        out_shape=jax.ShapeDtypeStruct((n_fs * n_tp, capacity, ratio * part), BF16),
        scratch_shapes=[
            VMEM((slots, n_tp * cols), BF16),
            VMEM((n_fs * part, n_tp * cols), BF16),
        ],
        compiler_params=GRANT,
        name="down",
    )(*hiddens, *chunks)


def finish(info, back, n_fs, batch, pieces, down_half):
    n_tp = len(pieces)
    part, cols = pieces[0].shape[1:]
    capacity, wide = back.shape[1:]
    ratio = wide // part
    rows = info.shape[0]
    group = n_fs // ratio

    def kernel(info_ref, back_ref, *refs):
        piece_refs = refs[:n_tp]
        out, down_ref, block_ref, back_rows, sems = refs[n_tp + 1 :]
        own, lane = own_places()
        copies = gather_blocks(batch, piece_refs, own, lane, block_ref, down_ref, sems)
        for e in range(n_fs):
            at = (e // ratio) * capacity
            for j in range(n_tp):
                back_rows[e % ratio, at : at + capacity, j * wide : (j + 1) * wide] = back_ref[
                    e * n_tp + j
                ]
        values = info_ref[...]
        places = lax.broadcasted_iota(jnp.int32, (2 * rows, group * capacity), 1).astype(F32)
        halves = []
        for k in range(ratio):
            both = jnp.concatenate(
                [values[:, 2 + 2 * k : 3 + 2 * k], values[:, 3 + 2 * k : 4 + 2 * k]], axis=0
            )
            pick = (both == places).astype(F32).astype(BF16)
            halves.append(jnp.dot(pick, back_rows[k], preferred_element_type=F32))
        for y in range(ratio):
            for j in range(n_tp):
                total = sum(
                    halves[k][:, j * wide + (y ^ k) * part : j * wide + ((y ^ k) + 1) * part]
                    for k in range(ratio)
                )
                value = values[:, 0:1] * total[:rows] + values[:, 1:2] * total[rows:]
                at = (y * n_tp + j) * part
                out[:, at : at + part] = value.astype(BF16)
        for copy in copies:
            copy.wait()

    return pl.pallas_call(
        kernel,
        in_specs=[whole(VMEM)] * (2 + n_tp) + [whole(ANY)],
        out_specs=[whole(VMEM), whole(ANY)],
        out_shape=[
            jax.ShapeDtypeStruct((rows, n_tp * wide), BF16),
            jax.ShapeDtypeStruct(down_half.shape, BF16),
        ],
        scratch_shapes=[
            VMEM((len(batch), n_tp * part, cols), BF16),
            VMEM((ratio, group * capacity, n_tp * wide), BF16),
            pltpu.SemaphoreType.DMA((len(batch),)),
        ],
        input_output_aliases={2 + n_tp: 1},
        compiler_params=GRANT,
        name="finish",
    )(info, back, *pieces, down_half)


def exchange_body(
    n_fs,
    n_tp,
    tokens,
    norm_gain,
    gate_weight,
    up_weight,
    down_weight,
    route_ids,
    group_weight,
    logit_gap,
):
    experts = gate_weight.shape[0]
    tok_rows = tokens.shape[0]
    capacity = max(2, (3 * tok_rows + experts - 1) // experts)
    block = gate_weight.shape[1]
    far, near = halves_of(n_fs)
    early = far[: n_fs // 4]
    later = far[n_fs // 4 :] + near
    batches = [near + early, far[n_fs // 4 :]]
    row_order = batches[0] + batches[1]

    def swap_fs(value, s):
        if s == 0:
            return value
        return lax.ppermute(value, "fs", [(n, n ^ s) for n in range(n_fs)])

    def swap_tp(value, s):
        if s == 0:
            return value
        return lax.ppermute(value, "tp", [(n, n ^ s) for n in range(n_tp)])

    gain = norm_gain[None, :]
    gate_weight, up_weight, down_weight = (
        pltpu.with_memory_space_constraint(value, pltpu.HBM)
        for value in (gate_weight, up_weight, down_weight)
    )
    weights = (gate_weight, up_weight)
    info, later_rows, *early_chunks = start_first(
        early,
        later,
        *(
            pltpu.with_memory_space_constraint(value, pltpu.HBM)
            for value in (
                route_ids.T,
                group_weight[None, :],
                logit_gap[None, :],
                tokens,
                gain,
            )
        ),
        weights,
        capacity,
        n_fs // n_tp,
    )
    later_chunks = start_later(later, later_rows, gain, weights)
    local = dict(zip(early + later, list(early_chunks) + list(later_chunks)))
    chunks = [swap_fs(local[s], s) for s in range(n_fs)]

    down_parts = cast_rows(down_weight, n_tp)
    down_parts = [swap_tp(down_parts[t], t) for t in range(n_tp)]
    down_local = regroup(down_parts)
    down_chunks = [swap_fs(down_local[s], s) for s in range(n_fs)]

    parts, quarters = [], []
    for batch in batches:
        rows = slot_rows_of([chunks[s] for s in batch], 2 * block, capacity)
        parts.append([swap_tp(rows, t) for t in range(n_tp)])
    for batch in (near, far):
        pieces = regroup([down_chunks[s] for s in batch])
        quarters.append([swap_tp(pieces[t], t) for t in range(n_tp)])

    hidden = gate_up(parts, chunks, block)
    hiddens = [swap_tp(hidden, t) for t in range(n_tp)]
    rows = down(row_order, hiddens, down_chunks, capacity)
    back = lax.all_to_all(rows, ("fs", "tp"), split_axis=0, concat_axis=0, tiled=True)
    gate_out, up_out, down_half = store(chunks, block, near, quarters[0])
    mixed, down_out = finish(info, back, n_fs, far, quarters[1], down_half)
    return gate_out, up_out, down_out, mixed


def halves_of(n_fs):
    steps = [s ^ (n_fs - 1) for s in range(n_fs)]
    return steps[: n_fs // 2], steps[n_fs // 2 :]


def slot_tables(route_ids, experts, capacity):
    row_count = route_ids.shape[0]
    pair_count = 2 * row_count
    flat_ids = route_ids.reshape(pair_count)
    onehot = (flat_ids[:, None] == jnp.arange(experts, dtype=jnp.int32)[None, :]).astype(
        jnp.bfloat16
    )
    positions = jnp.arange(pair_count, dtype=jnp.int32)
    below_mask = (positions[:, None] > positions[None, :]).astype(jnp.bfloat16)
    before = jnp.dot(below_mask, onehot, preferred_element_type=jnp.float32)
    ranked = jnp.sum(before * onehot.astype(jnp.float32), axis=1).astype(jnp.int32)
    return (flat_ids * capacity + ranked).reshape(row_count, 2)


def first_products(slot_rows, gate_cols, up_cols):
    shard_cols = lax.all_gather(slot_rows, "tp", axis=1, tiled=True)
    return (
        jnp.dot(shard_cols, gate_cols, preferred_element_type=jnp.float32),
        jnp.dot(shard_cols, up_cols, preferred_element_type=jnp.float32),
    )


def body(
    tokens, norm_gain, gate_weight, up_weight, down_weight, route_ids, group_weight, logit_gap
):
    experts = gate_weight.shape[0]
    tok_rows = tokens.shape[0]
    capacity = max(2, (3 * tok_rows + experts - 1) // experts)
    folded = norm_gain[None, :, None]
    gate_local = (gate_weight * folded).astype(jnp.bfloat16)
    up_local = (up_weight * folded).astype(jnp.bfloat16)
    down_local = down_weight.astype(jnp.bfloat16)
    slot_ids = slot_tables(route_ids, experts, capacity)
    slot_range = jnp.arange(experts * capacity, dtype=jnp.int32)
    matches = (slot_ids[None, :, :] == slot_range[:, None, None]).astype(jnp.int32)
    dispatch = jnp.sum(matches, axis=2).astype(jnp.bfloat16)
    outgoing = jnp.dot(dispatch, tokens, preferred_element_type=jnp.float32).astype(jnp.bfloat16)
    outgoing = outgoing.reshape(experts, capacity, tokens.shape[1])
    arrived = lax.all_to_all(outgoing, "fs", split_axis=0, concat_axis=0, tiled=True)
    slot_rows = arrived.reshape(experts * capacity, tokens.shape[1])
    gate_out, up_out, down_out = (
        lax.all_to_all(gate_local, "fs", split_axis=0, concat_axis=1, tiled=True),
        lax.all_to_all(up_local, "fs", split_axis=0, concat_axis=1, tiled=True),
        lax.all_to_all(down_local, "fs", split_axis=0, concat_axis=1, tiled=True),
    )
    gate_acc, up_acc = first_products(slot_rows, gate_out[0], up_out[0])
    hidden = (jax.nn.silu(gate_acc) * up_acc).astype(jnp.bfloat16)
    partial_value = lax.dot_general(
        hidden, down_out[0], (((1,), (1,)), ((), ())), preferred_element_type=jnp.float32
    )
    summed = lax.psum_scatter(
        partial_value.astype(jnp.bfloat16), "tp", scatter_dimension=1, tiled=True
    )
    returned = lax.all_to_all(
        summed.reshape(experts, capacity, summed.shape[1]),
        "fs",
        split_axis=0,
        concat_axis=0,
        tiled=True,
    )
    back_rows = returned.reshape(experts * capacity, summed.shape[1])
    pick_first = (slot_ids[:, 0:1] == slot_range[None, :]).astype(jnp.bfloat16)
    pick_second = (slot_ids[:, 1:2] == slot_range[None, :]).astype(jnp.bfloat16)
    first_vals = jnp.dot(pick_first, back_rows, preferred_element_type=jnp.float32)
    second_vals = jnp.dot(pick_second, back_rows, preferred_element_type=jnp.float32)
    first_weight = group_weight * jax.nn.sigmoid(logit_gap)
    second_weight = group_weight * jax.nn.sigmoid(-logit_gap)
    mixed = (first_weight[:, None] * first_vals + second_weight[:, None] * second_vals).astype(
        jnp.bfloat16
    )
    return (gate_out, up_out, down_out, mixed)


def solution(mesh):
    n_fs, n_tp = mesh.shape["fs"], mesh.shape["tp"]
    small = n_fs <= 16 and n_fs % n_tp == 0 and n_fs & (n_fs - 1) == 0

    def step(*args):
        if not small:
            return body(*args)
        return exchange_body(n_fs, n_tp, *args)

    return jax.shard_map(
        step,
        mesh=mesh,
        in_specs=(
            P("fs", "tp"),
            P("fs"),
            P(None, "fs", "tp"),
            P(None, "fs", "tp"),
            P(None, "fs", "tp"),
            P("fs", None),
            P("fs"),
            P("fs"),
        ),
        out_specs=(P("fs", None, "tp"), P("fs", None, "tp"), P("fs", None, "tp"), P("fs", "tp")),
        check_vma=False,
    )
```

```python
import jax
import jax.numpy as jnp
from jax import lax
from jax.experimental import pallas as pl
from jax.experimental.pallas import tpu as pltpu
from jax.sharding import PartitionSpec as P


BF16 = jnp.bfloat16
F32 = jnp.float32


GRANT = pltpu.CompilerParams(vmem_limit_bytes=8 * 1024 * 1024)
VMEM = pltpu.VMEM
ANY = pl.ANY


def whole(space):
    return pl.BlockSpec(memory_space=space)


def column(row):
    n = row.shape[1]
    same = lax.broadcasted_iota(jnp.int32, (n, n), 0) == lax.broadcasted_iota(jnp.int32, (n, n), 1)
    return jnp.sum(jnp.where(same, row, 0.0), axis=1, keepdims=True)


def own_places():
    return lax.axis_index("fs").astype(jnp.int32), lax.axis_index("tp").astype(jnp.int32)


def put_rows(target, base, rows):
    capacity, features = rows.shape
    cols = target.shape[1]
    for c in range(features // cols):
        at = base + c * capacity
        target[at : at + capacity, :] = rows[:, c * cols : (c + 1) * cols]


def fetch(pairs, sems):
    copies = []
    for n, (source, target) in enumerate(pairs):
        copy = pltpu.make_async_copy(source, target, sems.at[n])
        copy.start()
        copies.append(copy)
    return copies


def start_first(
    steps, later, routes, group_weight, logit_gap, tokens, gain, weights, capacity, ratio
):
    tok_rows, features = tokens.shape
    experts, block, cols = weights[0].shape
    stack, count = len(weights), len(steps)
    lanes = features // cols
    height = stack * block + lanes * capacity
    small = (routes, group_weight, logit_gap, tokens, gain)

    def kernel(*refs):
        small_in = refs[: len(small)]
        sources = refs[len(small) : len(small) + stack]
        at = len(small) + stack
        info_ref, later_ref = refs[at : at + 2]
        targets = refs[at + 2 : at + 2 + count]
        small_refs = refs[at + 2 + count : at + 2 + count + len(small)]
        buffer, small_sems, sems = refs[at + 2 + count + len(small) :]
        route_ref, group_ref, gap_ref, tok_ref, gain_ref = small_refs
        own, _ = own_places()
        small_copies = fetch(list(zip(small_in, small_refs)), small_sems)
        order = [(n, w) for n in range(count) for w in range(stack)]
        copies = fetch(
            [(sources[w].at[own ^ steps[n]], buffer.at[n, w]) for n, w in order], sems
        )
        for copy in small_copies:
            copy.wait()
        first = route_ref[0:1, :]
        second = route_ref[1:2, :]
        names = lax.broadcasted_iota(jnp.int32, (experts, tok_rows), 0)
        hit_first = (names == first).astype(F32)
        hit_second = (names == second).astype(F32)
        shape = (tok_rows, tok_rows)
        above = lax.broadcasted_iota(jnp.int32, shape, 0) < lax.broadcasted_iota(jnp.int32, shape, 1)
        before = jnp.dot(
            (hit_first + hit_second).astype(BF16),
            above.astype(F32).astype(BF16),
            preferred_element_type=F32,
        )
        rank_first = jnp.sum(before * hit_first, axis=0, keepdims=True).astype(jnp.int32)
        rank_second = jnp.sum(before * hit_second, axis=0, keepdims=True).astype(jnp.int32)
        slots = lax.broadcasted_iota(jnp.int32, (experts * capacity, tok_rows), 0)
        there_first = (first ^ own) * capacity + rank_first
        there_second = (second ^ own) * capacity + rank_second
        chosen = ((there_first == slots) | (there_second == slots)).astype(F32).astype(BF16)
        outgoing = jnp.dot(chosen, tok_ref[...], preferred_element_type=F32).astype(BF16)
        for n, s in enumerate(steps):
            put_rows(targets[n], stack * block, outgoing[s * capacity : (s + 1) * capacity])
        for n, s in enumerate(later):
            put_rows(later_ref.at[n], 0, outgoing[s * capacity : (s + 1) * capacity])
        gap = gap_ref[...]
        group = group_ref[...]
        info_ref[:, 0:1] = column(group * jax.nn.sigmoid(gap))
        info_ref[:, 1:2] = column(group * jax.nn.sigmoid(-gap))
        for k in range(ratio):
            for c, (name, rank) in enumerate(((first, rank_first), (second, rank_second))):
                place = (name // ratio) * capacity + rank
                place = jnp.where(name % ratio == k, place, -1)
                info_ref[:, 2 + 2 * k + c : 3 + 2 * k + c] = column(place.astype(F32))
        factor = column(gain_ref[...])
        for (n, w), copy in zip(order, copies):
            copy.wait()
            targets[n][w * block : (w + 1) * block, :] = (buffer[n, w] * factor).astype(BF16)

    return pl.pallas_call(
        kernel,
        in_specs=[whole(ANY)] * (len(small) + stack),
        out_specs=[whole(VMEM)] * (2 + count),
        out_shape=[
            jax.ShapeDtypeStruct((tok_rows, 2 + 2 * ratio), F32),
            jax.ShapeDtypeStruct((len(later), lanes * capacity, cols), BF16),
        ]
        + [jax.ShapeDtypeStruct((height, cols), BF16)] * count,
        scratch_shapes=[VMEM(value.shape, value.dtype) for value in small]
        + [
            VMEM((count, stack, block, cols), F32),
            pltpu.SemaphoreType.DMA((len(small),)),
            pltpu.SemaphoreType.DMA((count * stack,)),
        ],
        compiler_params=GRANT,
        name="start_first",
    )(*small, *weights)


def start_later(steps, later_rows, gain, weights):
    stack, count = len(weights), len(steps)
    block, cols = weights[0].shape[1:]
    tail = later_rows.shape[1]

    def kernel(rows_ref, gain_ref, *refs):
        sources = refs[:stack]
        targets = refs[stack : stack + count]
        buffer, sems = refs[stack + count :]
        own, _ = own_places()
        order = [(n, w) for n in range(count) for w in range(stack)]
        copies = fetch(
            [(sources[w].at[own ^ steps[n]], buffer.at[n, w]) for n, w in order], sems
        )
        factor = column(gain_ref[...])
        for n in range(count):
            targets[n][stack * block :, :] = rows_ref[n]
        for (n, w), copy in zip(order, copies):
            copy.wait()
            targets[n][w * block : (w + 1) * block, :] = (buffer[n, w] * factor).astype(BF16)

    return pl.pallas_call(
        kernel,
        in_specs=[whole(VMEM)] * 2 + [whole(ANY)] * stack,
        out_specs=[whole(VMEM)] * count,
        out_shape=[jax.ShapeDtypeStruct((stack * block + tail, cols), BF16)] * count,
        scratch_shapes=[
            VMEM((count, stack, block, cols), F32),
            pltpu.SemaphoreType.DMA((count * stack,)),
        ],
        compiler_params=GRANT,
        name="start_later",
    )(later_rows, gain, *weights)


def slot_rows_of(chunks, base, capacity):
    count = len(chunks)
    height, cols = chunks[0].shape
    lanes = (height - base) // capacity

    def kernel(*refs):
        out = refs[count]
        for n in range(count):
            for c in range(lanes):
                at = base + c * capacity
                out[n * capacity : (n + 1) * capacity, c * cols : (c + 1) * cols] = refs[n][
                    at : at + capacity, :
                ]

    return pl.pallas_call(
        kernel,
        in_specs=[whole(VMEM)] * count,
        out_specs=whole(VMEM),
        out_shape=jax.ShapeDtypeStruct((count * capacity, lanes * cols), BF16),
        compiler_params=GRANT,
        name="slot_rows",
    )(*chunks)


def cast_rows(weight, n_tp):
    experts, rows, cols = weight.shape
    part = rows // n_tp

    def kernel(source, *refs):
        targets = refs[:n_tp]
        buffer, sems = refs[n_tp:]
        own, lane = own_places()
        copies = fetch([(source.at[own ^ s], buffer.at[s]) for s in range(experts)], sems)
        for s, copy in enumerate(copies):
            copy.wait()
            for t in range(n_tp):
                start = pl.multiple_of((lane ^ t) * part, part)
                targets[t][s] = buffer[s, pl.ds(start, part), :].astype(BF16)

    return pl.pallas_call(
        kernel,
        in_specs=[whole(ANY)],
        out_specs=[whole(VMEM)] * n_tp,
        out_shape=[jax.ShapeDtypeStruct((experts, part, cols), BF16)] * n_tp,
        scratch_shapes=[
            VMEM((experts, rows, cols), F32),
            pltpu.SemaphoreType.DMA((experts,)),
        ],
        compiler_params=GRANT,
        name="cast_rows",
    )(weight)


def regroup(parts):
    inner, outer = len(parts), parts[0].shape[0]

    def kernel(*refs):
        for s in range(outer):
            for t in range(inner):
                refs[inner + s][t] = refs[t][s]

    return pl.pallas_call(
        kernel,
        in_specs=[whole(VMEM)] * inner,
        out_specs=[whole(VMEM)] * outer,
        out_shape=[jax.ShapeDtypeStruct((inner,) + parts[0].shape[1:], parts[0].dtype)] * outer,
        compiler_params=GRANT,
        name="regroup",
    )(*parts)


def gate_up(parts, chunks, block):
    n_fs, n_tp = len(chunks), len(parts[0])
    ratio = n_fs // n_tp
    cols = chunks[0].shape[1]
    counts = [batch[0].shape[0] for batch in parts]
    slots = sum(counts)
    flat = [piece for batch in parts for piece in batch]

    def kernel(*refs):
        piece_refs = refs[: len(flat)]
        chunk_refs = refs[len(flat) : len(flat) + n_fs]
        hidden_ref, rows_ref = refs[len(flat) + n_fs :]
        own, lane = own_places()
        at = 0
        for k, count in enumerate(counts):
            for t in range(n_tp):
                for h in range(ratio):
                    rows_ref[(lane ^ t) * ratio + h, at : at + count] = piece_refs[k * n_tp + t][
                        :, h * block : (h + 1) * block
                    ]
            at += count
        gate_acc = jnp.zeros((slots, cols), F32)
        up_acc = jnp.zeros((slots, cols), F32)
        for s in range(n_fs):
            rows = rows_ref[own ^ s]
            gate_acc += jnp.dot(rows, chunk_refs[s][:block], preferred_element_type=F32)
            up_acc += jnp.dot(rows, chunk_refs[s][block : 2 * block], preferred_element_type=F32)
        hidden_ref[...] = (gate_acc / (1.0 + jnp.exp(-gate_acc)) * up_acc).astype(BF16)

    return pl.pallas_call(
        kernel,
        in_specs=[whole(VMEM)] * (len(flat) + n_fs),
        out_specs=whole(VMEM),
        out_shape=jax.ShapeDtypeStruct((slots, cols), BF16),
        scratch_shapes=[VMEM((n_fs, slots, block), BF16)],
        compiler_params=GRANT,
        name="gate_up",
    )(*flat, *chunks)


def gather_blocks(batch, pieces, own, lane, block_ref, down_ref, sems):
    n_tp = len(pieces)
    part = pieces[0].shape[1]
    block = n_tp * part
    copies = []
    for n, s in enumerate(batch):
        for t in range(n_tp):
            at = pl.multiple_of((lane ^ t) * part, part)
            block_ref[n, pl.ds(at, part), :] = pieces[t][n]
        start = pl.multiple_of((own ^ s) * block, block)
        copy = pltpu.make_async_copy(
            block_ref.at[n], down_ref.at[0, pl.ds(start, block)], sems.at[n]
        )
        copy.start()
        copies.append(copy)
    return copies


def store(chunks, block, batch, pieces):
    n_fs, n_tp = len(chunks), len(pieces)
    cols = chunks[0].shape[1]

    def kernel(*refs):
        piece_refs = refs[n_fs : n_fs + n_tp]
        outs = refs[n_fs + n_tp : n_fs + n_tp + 3]
        block_ref, sems, down_sems = refs[n_fs + n_tp + 3 :]
        own, lane = own_places()
        copies = gather_blocks(batch, piece_refs, own, lane, block_ref, outs[2], down_sems)
        for s in range(n_fs):
            start = pl.multiple_of((own ^ s) * block, block)
            for w in range(2):
                copy = pltpu.make_async_copy(
                    refs[s].at[pl.ds(w * block, block)],
                    outs[w].at[0, pl.ds(start, block)],
                    sems.at[s, w],
                )
                copy.start()
                copies.append(copy)
        for copy in copies:
            copy.wait()

    full = jax.ShapeDtypeStruct((1, n_fs * block, cols), BF16)
    return pl.pallas_call(
        kernel,
        in_specs=[whole(VMEM)] * (n_fs + n_tp),
        out_specs=[whole(ANY)] * 3,
        out_shape=[full] * 3,
        scratch_shapes=[
            VMEM((len(batch), block, cols), BF16),
            pltpu.SemaphoreType.DMA((n_fs, 2)),
            pltpu.SemaphoreType.DMA((len(batch),)),
        ],
        compiler_params=GRANT,
        name="store",
    )(*chunks, *pieces)


def down(row_order, hiddens, chunks, capacity):
    n_tp, n_fs = len(hiddens), len(chunks)
    ratio = n_fs // n_tp
    slots, cols = hiddens[0].shape
    part = chunks[0].shape[1]

    def kernel(*refs):
        hidden_refs = refs[:n_tp]
        chunk_refs = refs[n_tp : n_tp + n_fs]
        out_ref, hidden_ref, all_ref, value_ref, sems = refs[n_tp + n_fs :]
        own, _ = own_places()
        wide = ratio * part
        for t in range(n_tp):
            hidden_ref[:, t * cols : (t + 1) * cols] = hidden_refs[t][...]
        copies = []
        for m in range(n_tp):
            for s in range(m * ratio, (m + 1) * ratio):
                for t in range(n_tp):
                    all_ref[s * part : (s + 1) * part, t * cols : (t + 1) * cols] = chunk_refs[s][t]
            value = lax.dot_general(
                hidden_ref[...],
                all_ref[m * wide : (m + 1) * wide],
                (((1,), (1,)), ((), ())),
                preferred_element_type=F32,
            )
            for k, s in enumerate(row_order):
                value_ref[m, own ^ s] = value[k * capacity : (k + 1) * capacity].astype(BF16)
            quarter = (own // ratio) ^ m
            copy = pltpu.make_async_copy(value_ref.at[m], out_ref.at[:, quarter], sems.at[m])
            copy.start()
            copies.append(copy)
        for copy in copies:
            copy.wait()

    return pl.pallas_call(
        kernel,
        in_specs=[whole(VMEM)] * (n_tp + n_fs),
        out_specs=whole(ANY),
        out_shape=jax.ShapeDtypeStruct((n_fs, n_tp, capacity, ratio * part), BF16),
        scratch_shapes=[
            VMEM((slots, n_tp * cols), BF16),
            VMEM((n_fs * part, n_tp * cols), BF16),
            VMEM((n_tp, n_fs, capacity, ratio * part), BF16),
            pltpu.SemaphoreType.DMA((n_tp,)),
        ],
        compiler_params=GRANT,
        name="down",
    )(*hiddens, *chunks)


def finish(info, back, n_fs, batch, pieces, down_half):
    n_tp = len(pieces)
    part, cols = pieces[0].shape[1:]
    capacity, wide = back.shape[1:]
    ratio = wide // part
    rows = info.shape[0]
    group = n_fs // ratio

    def kernel(info_ref, back_ref, *refs):
        piece_refs = refs[:n_tp]
        mixed_ref, down_ref, block_ref, back_rows, out, sems, out_sem = refs[n_tp + 1 :]
        own, lane = own_places()
        copies = gather_blocks(batch, piece_refs, own, lane, block_ref, down_ref, sems)
        for e in range(n_fs):
            at = (e // ratio) * capacity
            for j in range(n_tp):
                back_rows[e % ratio, at : at + capacity, j * wide : (j + 1) * wide] = back_ref[
                    e * n_tp + j
                ]
        values = info_ref[...]
        places = lax.broadcasted_iota(jnp.int32, (2 * rows, group * capacity), 1).astype(F32)
        halves = []
        for k in range(ratio):
            both = jnp.concatenate(
                [values[:, 2 + 2 * k : 3 + 2 * k], values[:, 3 + 2 * k : 4 + 2 * k]], axis=0
            )
            pick = (both == places).astype(F32).astype(BF16)
            halves.append(jnp.dot(pick, back_rows[k], preferred_element_type=F32))
        for y in range(ratio):
            for j in range(n_tp):
                total = sum(
                    halves[k][:, j * wide + (y ^ k) * part : j * wide + ((y ^ k) + 1) * part]
                    for k in range(ratio)
                )
                value = values[:, 0:1] * total[:rows] + values[:, 1:2] * total[rows:]
                at = (y * n_tp + j) * part
                out[:, at : at + part] = value.astype(BF16)
        copies += fetch([(out, mixed_ref)], out_sem)
        for copy in copies:
            copy.wait()

    return pl.pallas_call(
        kernel,
        in_specs=[whole(VMEM)] * (2 + n_tp) + [whole(ANY)],
        out_specs=[whole(ANY), whole(ANY)],
        out_shape=[
            jax.ShapeDtypeStruct((rows, n_tp * wide), BF16),
            jax.ShapeDtypeStruct(down_half.shape, BF16),
        ],
        scratch_shapes=[
            VMEM((len(batch), n_tp * part, cols), BF16),
            VMEM((ratio, group * capacity, n_tp * wide), BF16),
            VMEM((rows, n_tp * wide), BF16),
            pltpu.SemaphoreType.DMA((len(batch),)),
            pltpu.SemaphoreType.DMA((1,)),
        ],
        input_output_aliases={2 + n_tp: 1},
        compiler_params=GRANT,
        name="finish",
    )(info, back, *pieces, down_half)


def exchange_body(
    n_fs,
    n_tp,
    tokens,
    norm_gain,
    gate_weight,
    up_weight,
    down_weight,
    route_ids,
    group_weight,
    logit_gap,
):
    experts = gate_weight.shape[0]
    tok_rows = tokens.shape[0]
    capacity = max(2, (3 * tok_rows + experts - 1) // experts)
    block = gate_weight.shape[1]
    far, near = halves_of(n_fs)
    early = far[: n_fs // 4]
    later = far[n_fs // 4 :] + near
    batches = [near + early, far[n_fs // 4 :]]
    row_order = batches[0] + batches[1]

    def swap_fs(value, s):
        if s == 0:
            return value
        return lax.ppermute(value, "fs", [(n, n ^ s) for n in range(n_fs)])

    def swap_tp(value, s):
        if s == 0:
            return value
        return lax.ppermute(value, "tp", [(n, n ^ s) for n in range(n_tp)])

    def gather_tp(value):
        parts = {0: value}
        step = n_tp
        while step > 1:
            step //= 2
            for t in sorted(parts):
                parts[t + step] = lax.ppermute(parts[t], "tp", [(n, n ^ step) for n in range(n_tp)])
        return [parts[t] for t in range(n_tp)]

    gain = norm_gain[None, :]
    gate_weight, up_weight, down_weight = (
        pltpu.with_memory_space_constraint(value, pltpu.HBM)
        for value in (gate_weight, up_weight, down_weight)
    )
    weights = (gate_weight, up_weight)
    info, later_rows, *early_chunks = start_first(
        early,
        later,
        *(
            pltpu.with_memory_space_constraint(value, pltpu.HBM)
            for value in (
                route_ids.T,
                group_weight[None, :],
                logit_gap[None, :],
                tokens,
                gain,
            )
        ),
        weights,
        capacity,
        n_fs // n_tp,
    )
    later_chunks = start_later(later, later_rows, gain, weights)
    local = dict(zip(early + later, list(early_chunks) + list(later_chunks)))
    chunks = [swap_fs(local[s], s) for s in range(n_fs)]

    down_parts = cast_rows(down_weight, n_tp)
    down_parts = [swap_tp(down_parts[t], t) for t in range(n_tp)]
    down_local = regroup(down_parts)
    down_chunks = [swap_fs(down_local[s], s) for s in range(n_fs)]

    parts, quarters = [], []
    for batch in batches:
        rows = slot_rows_of([chunks[s] for s in batch], 2 * block, capacity)
        parts.append(gather_tp(rows))
    for batch in batches:
        pieces = regroup([down_chunks[s] for s in batch])
        quarters.append([swap_tp(pieces[t], t) for t in range(n_tp)])

    hidden = gate_up(parts, chunks, block)
    hiddens = gather_tp(hidden)
    rows = down(row_order, hiddens, down_chunks, capacity)
    rows = rows.reshape(n_fs * n_tp, *rows.shape[2:])
    back = lax.all_to_all(rows, ("fs", "tp"), split_axis=0, concat_axis=0, tiled=True)
    gate_out, up_out, down_half = store(chunks, block, batches[0], quarters[0])
    mixed, down_out = finish(info, back, n_fs, batches[1], quarters[1], down_half)
    return gate_out, up_out, down_out, mixed


def halves_of(n_fs):
    steps = [s ^ (n_fs - 1) for s in range(n_fs)]
    return steps[: n_fs // 2], steps[n_fs // 2 :]


def slot_tables(route_ids, experts, capacity):
    row_count = route_ids.shape[0]
    pair_count = 2 * row_count
    flat_ids = route_ids.reshape(pair_count)
    onehot = (flat_ids[:, None] == jnp.arange(experts, dtype=jnp.int32)[None, :]).astype(
        jnp.bfloat16
    )
    positions = jnp.arange(pair_count, dtype=jnp.int32)
    below_mask = (positions[:, None] > positions[None, :]).astype(jnp.bfloat16)
    before = jnp.dot(below_mask, onehot, preferred_element_type=jnp.float32)
    ranked = jnp.sum(before * onehot.astype(jnp.float32), axis=1).astype(jnp.int32)
    return (flat_ids * capacity + ranked).reshape(row_count, 2)


def first_products(slot_rows, gate_cols, up_cols):
    shard_cols = lax.all_gather(slot_rows, "tp", axis=1, tiled=True)
    return (
        jnp.dot(shard_cols, gate_cols, preferred_element_type=jnp.float32),
        jnp.dot(shard_cols, up_cols, preferred_element_type=jnp.float32),
    )


def body(
    tokens, norm_gain, gate_weight, up_weight, down_weight, route_ids, group_weight, logit_gap
):
    experts = gate_weight.shape[0]
    tok_rows = tokens.shape[0]
    capacity = max(2, (3 * tok_rows + experts - 1) // experts)
    folded = norm_gain[None, :, None]
    gate_local = (gate_weight * folded).astype(jnp.bfloat16)
    up_local = (up_weight * folded).astype(jnp.bfloat16)
    down_local = down_weight.astype(jnp.bfloat16)
    slot_ids = slot_tables(route_ids, experts, capacity)
    slot_range = jnp.arange(experts * capacity, dtype=jnp.int32)
    matches = (slot_ids[None, :, :] == slot_range[:, None, None]).astype(jnp.int32)
    dispatch = jnp.sum(matches, axis=2).astype(jnp.bfloat16)
    outgoing = jnp.dot(dispatch, tokens, preferred_element_type=jnp.float32).astype(jnp.bfloat16)
    outgoing = outgoing.reshape(experts, capacity, tokens.shape[1])
    arrived = lax.all_to_all(outgoing, "fs", split_axis=0, concat_axis=0, tiled=True)
    slot_rows = arrived.reshape(experts * capacity, tokens.shape[1])
    gate_out, up_out, down_out = (
        lax.all_to_all(gate_local, "fs", split_axis=0, concat_axis=1, tiled=True),
        lax.all_to_all(up_local, "fs", split_axis=0, concat_axis=1, tiled=True),
        lax.all_to_all(down_local, "fs", split_axis=0, concat_axis=1, tiled=True),
    )
    gate_acc, up_acc = first_products(slot_rows, gate_out[0], up_out[0])
    hidden = (jax.nn.silu(gate_acc) * up_acc).astype(jnp.bfloat16)
    partial_value = lax.dot_general(
        hidden, down_out[0], (((1,), (1,)), ((), ())), preferred_element_type=jnp.float32
    )
    summed = lax.psum_scatter(
        partial_value.astype(jnp.bfloat16), "tp", scatter_dimension=1, tiled=True
    )
    returned = lax.all_to_all(
        summed.reshape(experts, capacity, summed.shape[1]),
        "fs",
        split_axis=0,
        concat_axis=0,
        tiled=True,
    )
    back_rows = returned.reshape(experts * capacity, summed.shape[1])
    pick_first = (slot_ids[:, 0:1] == slot_range[None, :]).astype(jnp.bfloat16)
    pick_second = (slot_ids[:, 1:2] == slot_range[None, :]).astype(jnp.bfloat16)
    first_vals = jnp.dot(pick_first, back_rows, preferred_element_type=jnp.float32)
    second_vals = jnp.dot(pick_second, back_rows, preferred_element_type=jnp.float32)
    first_weight = group_weight * jax.nn.sigmoid(logit_gap)
    second_weight = group_weight * jax.nn.sigmoid(-logit_gap)
    mixed = (first_weight[:, None] * first_vals + second_weight[:, None] * second_vals).astype(
        jnp.bfloat16
    )
    return (gate_out, up_out, down_out, mixed)


def solution(mesh):
    n_fs, n_tp = mesh.shape["fs"], mesh.shape["tp"]
    small = n_fs <= 16 and n_fs % n_tp == 0 and n_fs & (n_fs - 1) == 0

    def step(*args):
        if not small:
            return body(*args)
        return exchange_body(n_fs, n_tp, *args)

    return jax.shard_map(
        step,
        mesh=mesh,
        in_specs=(
            P("fs", "tp"),
            P("fs"),
            P(None, "fs", "tp"),
            P(None, "fs", "tp"),
            P(None, "fs", "tp"),
            P("fs", None),
            P("fs"),
            P("fs"),
        ),
        out_specs=(P("fs", None, "tp"), P("fs", None, "tp"), P("fs", None, "tp"), P("fs", "tp")),
        check_vma=False,
    )
```

```python
import jax
import jax.numpy as jnp
from jax import lax
from jax.experimental import pallas as pl
from jax.experimental.pallas import tpu as pltpu
from jax.sharding import PartitionSpec as P


BF16 = jnp.bfloat16
F32 = jnp.float32


GRANT = pltpu.CompilerParams(vmem_limit_bytes=8 * 1024 * 1024)
VMEM = pltpu.VMEM
ANY = pl.ANY


def whole(space):
    return pl.BlockSpec(memory_space=space)


def column(row):
    n = row.shape[1]
    same = lax.broadcasted_iota(jnp.int32, (n, n), 0) == lax.broadcasted_iota(jnp.int32, (n, n), 1)
    return jnp.sum(jnp.where(same, row, 0.0), axis=1, keepdims=True)


def own_places():
    return lax.axis_index("fs").astype(jnp.int32), lax.axis_index("tp").astype(jnp.int32)


def put_rows(target, base, rows):
    capacity, features = rows.shape
    cols = target.shape[1]
    for c in range(features // cols):
        at = base + c * capacity
        target[at : at + capacity, :] = rows[:, c * cols : (c + 1) * cols]


def fetch(pairs, sems):
    copies = []
    for n, (source, target) in enumerate(pairs):
        copy = pltpu.make_async_copy(source, target, sems.at[n])
        copy.start()
        copies.append(copy)
    return copies


def start_first(
    steps, later, routes, group_weight, logit_gap, tokens, gain, weights, capacity, ratio
):
    tok_rows, features = tokens.shape
    experts, block, cols = weights[0].shape
    stack, count = len(weights), len(steps)
    lanes = features // cols
    height = stack * block + lanes * capacity
    small = (routes, group_weight, logit_gap, tokens, gain)

    def kernel(*refs):
        small_in = refs[: len(small)]
        sources = refs[len(small) : len(small) + stack]
        at = len(small) + stack
        info_ref, later_ref = refs[at : at + 2]
        targets = refs[at + 2 : at + 2 + count]
        small_refs = refs[at + 2 + count : at + 2 + count + len(small)]
        buffer, small_sems, sems = refs[at + 2 + count + len(small) :]
        route_ref, group_ref, gap_ref, tok_ref, gain_ref = small_refs
        own, _ = own_places()
        small_copies = fetch(list(zip(small_in, small_refs)), small_sems)
        order = [(n, w) for n in range(count) for w in range(stack)]
        copies = fetch(
            [(sources[w].at[own ^ steps[n]], buffer.at[n, w]) for n, w in order], sems
        )
        for copy in small_copies:
            copy.wait()
        first = route_ref[0:1, :]
        second = route_ref[1:2, :]
        names = lax.broadcasted_iota(jnp.int32, (experts, tok_rows), 0)
        hit_first = (names == first).astype(F32)
        hit_second = (names == second).astype(F32)
        shape = (tok_rows, tok_rows)
        above = lax.broadcasted_iota(jnp.int32, shape, 0) < lax.broadcasted_iota(jnp.int32, shape, 1)
        before = jnp.dot(
            (hit_first + hit_second).astype(BF16),
            above.astype(F32).astype(BF16),
            preferred_element_type=F32,
        )
        rank_first = jnp.sum(before * hit_first, axis=0, keepdims=True).astype(jnp.int32)
        rank_second = jnp.sum(before * hit_second, axis=0, keepdims=True).astype(jnp.int32)
        slots = lax.broadcasted_iota(jnp.int32, (experts * capacity, tok_rows), 0)
        there_first = (first ^ own) * capacity + rank_first
        there_second = (second ^ own) * capacity + rank_second
        chosen = ((there_first == slots) | (there_second == slots)).astype(F32).astype(BF16)
        outgoing = jnp.dot(chosen, tok_ref[...], preferred_element_type=F32).astype(BF16)
        for n, s in enumerate(steps):
            put_rows(targets[n], stack * block, outgoing[s * capacity : (s + 1) * capacity])
        for n, s in enumerate(later):
            put_rows(later_ref.at[n], 0, outgoing[s * capacity : (s + 1) * capacity])
        gap = gap_ref[...]
        group = group_ref[...]
        info_ref[:, 0:1] = column(group * jax.nn.sigmoid(gap))
        info_ref[:, 1:2] = column(group * jax.nn.sigmoid(-gap))
        for k in range(ratio):
            for c, (name, rank) in enumerate(((first, rank_first), (second, rank_second))):
                place = (name // ratio) * capacity + rank
                place = jnp.where(name % ratio == k, place, -1)
                info_ref[:, 2 + 2 * k + c : 3 + 2 * k + c] = column(place.astype(F32))
        factor = column(gain_ref[...])
        for (n, w), copy in zip(order, copies):
            copy.wait()
            targets[n][w * block : (w + 1) * block, :] = (buffer[n, w] * factor).astype(BF16)

    return pl.pallas_call(
        kernel,
        in_specs=[whole(ANY)] * (len(small) + stack),
        out_specs=[whole(VMEM)] * (2 + count),
        out_shape=[
            jax.ShapeDtypeStruct((tok_rows, 2 + 2 * ratio), F32),
            jax.ShapeDtypeStruct((len(later), lanes * capacity, cols), BF16),
        ]
        + [jax.ShapeDtypeStruct((height, cols), BF16)] * count,
        scratch_shapes=[VMEM(value.shape, value.dtype) for value in small]
        + [
            VMEM((count, stack, block, cols), F32),
            pltpu.SemaphoreType.DMA((len(small),)),
            pltpu.SemaphoreType.DMA((count * stack,)),
        ],
        compiler_params=GRANT,
        name="start_first",
    )(*small, *weights)


def start_later(steps, later_rows, gain, weights):
    stack, count = len(weights), len(steps)
    block, cols = weights[0].shape[1:]
    tail = later_rows.shape[1]

    def kernel(rows_ref, gain_in, *refs):
        sources = refs[:stack]
        targets = refs[stack : stack + count]
        buffer, gain_ref, sems, gain_sem = refs[stack + count :]
        own, _ = own_places()
        order = [(n, w) for n in range(count) for w in range(stack)]
        (gain_copy,) = fetch([(gain_in, gain_ref)], gain_sem)
        copies = fetch(
            [(sources[w].at[own ^ steps[n]], buffer.at[n, w]) for n, w in order], sems
        )
        for n in range(count):
            targets[n][stack * block :, :] = rows_ref[n]
        gain_copy.wait()
        factor = column(gain_ref[...])
        for (n, w), copy in zip(order, copies):
            copy.wait()
            targets[n][w * block : (w + 1) * block, :] = (buffer[n, w] * factor).astype(BF16)

    return pl.pallas_call(
        kernel,
        in_specs=[whole(VMEM)] + [whole(ANY)] * (1 + stack),
        out_specs=[whole(VMEM)] * count,
        out_shape=[jax.ShapeDtypeStruct((stack * block + tail, cols), BF16)] * count,
        scratch_shapes=[
            VMEM((count, stack, block, cols), F32),
            VMEM(gain.shape, F32),
            pltpu.SemaphoreType.DMA((count * stack,)),
            pltpu.SemaphoreType.DMA((1,)),
        ],
        compiler_params=GRANT,
        name="start_later",
    )(later_rows, gain, *weights)


def slot_rows_of(chunks, base, capacity):
    count = len(chunks)
    height, cols = chunks[0].shape
    lanes = (height - base) // capacity

    def kernel(*refs):
        out = refs[count]
        for n in range(count):
            for c in range(lanes):
                at = base + c * capacity
                out[n * capacity : (n + 1) * capacity, c * cols : (c + 1) * cols] = refs[n][
                    at : at + capacity, :
                ]

    return pl.pallas_call(
        kernel,
        in_specs=[whole(VMEM)] * count,
        out_specs=whole(VMEM),
        out_shape=jax.ShapeDtypeStruct((count * capacity, lanes * cols), BF16),
        compiler_params=GRANT,
        name="slot_rows",
    )(*chunks)


def cast_rows(weight, n_tp):
    experts, rows, cols = weight.shape
    part = rows // n_tp

    def kernel(source, *refs):
        targets = refs[:n_tp]
        buffer, sems = refs[n_tp:]
        own, lane = own_places()
        copies = fetch([(source.at[own ^ s], buffer.at[s]) for s in range(experts)], sems)
        for s, copy in enumerate(copies):
            copy.wait()
            for t in range(n_tp):
                start = pl.multiple_of((lane ^ t) * part, part)
                targets[t][s] = buffer[s, pl.ds(start, part), :].astype(BF16)

    return pl.pallas_call(
        kernel,
        in_specs=[whole(ANY)],
        out_specs=[whole(VMEM)] * n_tp,
        out_shape=[jax.ShapeDtypeStruct((experts, part, cols), BF16)] * n_tp,
        scratch_shapes=[
            VMEM((experts, rows, cols), F32),
            pltpu.SemaphoreType.DMA((experts,)),
        ],
        compiler_params=GRANT,
        name="cast_rows",
    )(weight)


def regroup(parts):
    inner, outer = len(parts), parts[0].shape[0]

    def kernel(*refs):
        for s in range(outer):
            for t in range(inner):
                refs[inner + s][t] = refs[t][s]

    return pl.pallas_call(
        kernel,
        in_specs=[whole(VMEM)] * inner,
        out_specs=[whole(VMEM)] * outer,
        out_shape=[jax.ShapeDtypeStruct((inner,) + parts[0].shape[1:], parts[0].dtype)] * outer,
        compiler_params=GRANT,
        name="regroup",
    )(*parts)


def gate_up(parts, chunks, block):
    n_fs, n_tp = len(chunks), len(parts[0])
    ratio = n_fs // n_tp
    cols = chunks[0].shape[1]
    counts = [batch[0].shape[0] for batch in parts]
    slots = sum(counts)
    flat = [piece for batch in parts for piece in batch]

    def kernel(*refs):
        piece_refs = refs[: len(flat)]
        chunk_refs = refs[len(flat) : len(flat) + n_fs]
        hidden_ref, rows_ref = refs[len(flat) + n_fs :]
        own, lane = own_places()
        at = 0
        for k, count in enumerate(counts):
            for t in range(n_tp):
                for h in range(ratio):
                    rows_ref[(lane ^ t) * ratio + h, at : at + count] = piece_refs[k * n_tp + t][
                        :, h * block : (h + 1) * block
                    ]
            at += count
        gate_acc = jnp.zeros((slots, cols), F32)
        up_acc = jnp.zeros((slots, cols), F32)
        for s in range(n_fs):
            rows = rows_ref[own ^ s]
            gate_acc += jnp.dot(rows, chunk_refs[s][:block], preferred_element_type=F32)
            up_acc += jnp.dot(rows, chunk_refs[s][block : 2 * block], preferred_element_type=F32)
        hidden_ref[...] = (gate_acc / (1.0 + jnp.exp(-gate_acc)) * up_acc).astype(BF16)

    return pl.pallas_call(
        kernel,
        in_specs=[whole(VMEM)] * (len(flat) + n_fs),
        out_specs=whole(VMEM),
        out_shape=jax.ShapeDtypeStruct((slots, cols), BF16),
        scratch_shapes=[VMEM((n_fs, slots, block), BF16)],
        compiler_params=GRANT,
        name="gate_up",
    )(*flat, *chunks)


def gather_blocks(batch, pieces, own, lane, block_ref, down_ref, sems):
    n_tp = len(pieces)
    part = pieces[0].shape[1]
    block = n_tp * part
    copies = []
    for n, s in enumerate(batch):
        for t in range(n_tp):
            at = pl.multiple_of((lane ^ t) * part, part)
            block_ref[n, pl.ds(at, part), :] = pieces[t][n]
        start = pl.multiple_of((own ^ s) * block, block)
        copy = pltpu.make_async_copy(
            block_ref.at[n], down_ref.at[0, pl.ds(start, block)], sems.at[n]
        )
        copy.start()
        copies.append(copy)
    return copies


def store(chunks, block, batch, pieces):
    n_fs, n_tp = len(chunks), len(pieces)
    cols = chunks[0].shape[1]

    def kernel(*refs):
        piece_refs = refs[n_fs : n_fs + n_tp]
        outs = refs[n_fs + n_tp : n_fs + n_tp + 3]
        block_ref, sems, down_sems = refs[n_fs + n_tp + 3 :]
        own, lane = own_places()
        copies = gather_blocks(batch, piece_refs, own, lane, block_ref, outs[2], down_sems)
        for s in range(n_fs):
            start = pl.multiple_of((own ^ s) * block, block)
            for w in range(2):
                copy = pltpu.make_async_copy(
                    refs[s].at[pl.ds(w * block, block)],
                    outs[w].at[0, pl.ds(start, block)],
                    sems.at[s, w],
                )
                copy.start()
                copies.append(copy)
        for copy in copies:
            copy.wait()

    full = jax.ShapeDtypeStruct((1, n_fs * block, cols), BF16)
    return pl.pallas_call(
        kernel,
        in_specs=[whole(VMEM)] * (n_fs + n_tp),
        out_specs=[whole(ANY)] * 3,
        out_shape=[full] * 3,
        scratch_shapes=[
            VMEM((len(batch), block, cols), BF16),
            pltpu.SemaphoreType.DMA((n_fs, 2)),
            pltpu.SemaphoreType.DMA((len(batch),)),
        ],
        compiler_params=GRANT,
        name="store",
    )(*chunks, *pieces)


def down(row_order, hiddens, chunks, capacity):
    n_tp, n_fs = len(hiddens), len(chunks)
    ratio = n_fs // n_tp
    slots, cols = hiddens[0].shape
    part = chunks[0].shape[1]

    def kernel(*refs):
        hidden_refs = refs[:n_tp]
        chunk_refs = refs[n_tp : n_tp + n_fs]
        out_ref, hidden_ref, all_ref, value_ref, sems = refs[n_tp + n_fs :]
        own, _ = own_places()
        wide = ratio * part
        for t in range(n_tp):
            hidden_ref[:, t * cols : (t + 1) * cols] = hidden_refs[t][...]
        copies = []
        for m in range(n_tp):
            for s in range(m * ratio, (m + 1) * ratio):
                for t in range(n_tp):
                    all_ref[s * part : (s + 1) * part, t * cols : (t + 1) * cols] = chunk_refs[s][t]
            value = lax.dot_general(
                hidden_ref[...],
                all_ref[m * wide : (m + 1) * wide],
                (((1,), (1,)), ((), ())),
                preferred_element_type=F32,
            )
            for k, s in enumerate(row_order):
                value_ref[m, own ^ s] = value[k * capacity : (k + 1) * capacity].astype(BF16)
            quarter = (own // ratio) ^ m
            copy = pltpu.make_async_copy(value_ref.at[m], out_ref.at[:, quarter], sems.at[m])
            copy.start()
            copies.append(copy)
        for copy in copies:
            copy.wait()

    return pl.pallas_call(
        kernel,
        in_specs=[whole(VMEM)] * (n_tp + n_fs),
        out_specs=whole(ANY),
        out_shape=jax.ShapeDtypeStruct((n_fs, n_tp, capacity, ratio * part), BF16),
        scratch_shapes=[
            VMEM((slots, n_tp * cols), BF16),
            VMEM((n_fs * part, n_tp * cols), BF16),
            VMEM((n_tp, n_fs, capacity, ratio * part), BF16),
            pltpu.SemaphoreType.DMA((n_tp,)),
        ],
        compiler_params=GRANT,
        name="down",
    )(*hiddens, *chunks)


def finish(info, back, n_fs, batch, pieces, down_half):
    n_tp = len(pieces)
    part, cols = pieces[0].shape[1:]
    capacity, wide = back.shape[1:]
    ratio = wide // part
    rows = info.shape[0]
    group = n_fs // ratio

    def kernel(info_ref, back_ref, *refs):
        piece_refs = refs[:n_tp]
        mixed_ref, down_ref, block_ref, back_rows, out, sems, out_sem = refs[n_tp + 1 :]
        own, lane = own_places()
        copies = gather_blocks(batch, piece_refs, own, lane, block_ref, down_ref, sems)
        for e in range(n_fs):
            at = (e // ratio) * capacity
            for j in range(n_tp):
                back_rows[e % ratio, at : at + capacity, j * wide : (j + 1) * wide] = back_ref[
                    e * n_tp + j
                ]
        values = info_ref[...]
        places = lax.broadcasted_iota(jnp.int32, (2 * rows, group * capacity), 1).astype(F32)
        halves = []
        for k in range(ratio):
            both = jnp.concatenate(
                [values[:, 2 + 2 * k : 3 + 2 * k], values[:, 3 + 2 * k : 4 + 2 * k]], axis=0
            )
            pick = (both == places).astype(F32).astype(BF16)
            halves.append(jnp.dot(pick, back_rows[k], preferred_element_type=F32))
        for y in range(ratio):
            for j in range(n_tp):
                total = sum(
                    halves[k][:, j * wide + (y ^ k) * part : j * wide + ((y ^ k) + 1) * part]
                    for k in range(ratio)
                )
                value = values[:, 0:1] * total[:rows] + values[:, 1:2] * total[rows:]
                at = (y * n_tp + j) * part
                out[:, at : at + part] = value.astype(BF16)
        copies += fetch([(out, mixed_ref)], out_sem)
        for copy in copies:
            copy.wait()

    return pl.pallas_call(
        kernel,
        in_specs=[whole(VMEM)] * (2 + n_tp) + [whole(ANY)],
        out_specs=[whole(ANY), whole(ANY)],
        out_shape=[
            jax.ShapeDtypeStruct((rows, n_tp * wide), BF16),
            jax.ShapeDtypeStruct(down_half.shape, BF16),
        ],
        scratch_shapes=[
            VMEM((len(batch), n_tp * part, cols), BF16),
            VMEM((ratio, group * capacity, n_tp * wide), BF16),
            VMEM((rows, n_tp * wide), BF16),
            pltpu.SemaphoreType.DMA((len(batch),)),
            pltpu.SemaphoreType.DMA((1,)),
        ],
        input_output_aliases={2 + n_tp: 1},
        compiler_params=GRANT,
        name="finish",
    )(info, back, *pieces, down_half)


def exchange_body(
    n_fs,
    n_tp,
    tokens,
    norm_gain,
    gate_weight,
    up_weight,
    down_weight,
    route_ids,
    group_weight,
    logit_gap,
):
    experts = gate_weight.shape[0]
    tok_rows = tokens.shape[0]
    capacity = max(2, (3 * tok_rows + experts - 1) // experts)
    block = gate_weight.shape[1]
    far, near = halves_of(n_fs)
    early, later = far[:1], far[1:] + near
    batches = [near + far[: n_fs // 4], far[n_fs // 4 :]]
    row_order = batches[0] + batches[1]

    def swap_fs(value, s):
        if s == 0:
            return value
        return lax.ppermute(value, "fs", [(n, n ^ s) for n in range(n_fs)])

    def swap_tp(value, s):
        if s == 0:
            return value
        return lax.ppermute(value, "tp", [(n, n ^ s) for n in range(n_tp)])

    def gather_tp(value):
        parts = {0: value}
        step = n_tp
        while step > 1:
            step //= 2
            for t in sorted(parts):
                parts[t + step] = lax.ppermute(parts[t], "tp", [(n, n ^ step) for n in range(n_tp)])
        return [parts[t] for t in range(n_tp)]

    gain = norm_gain[None, :]
    gate_weight, up_weight, down_weight = (
        pltpu.with_memory_space_constraint(value, pltpu.HBM)
        for value in (gate_weight, up_weight, down_weight)
    )
    weights = (gate_weight, up_weight)
    info, later_rows, *early_chunks = start_first(
        early,
        later,
        *(
            pltpu.with_memory_space_constraint(value, pltpu.HBM)
            for value in (
                route_ids.T,
                group_weight[None, :],
                logit_gap[None, :],
                tokens,
                gain,
            )
        ),
        weights,
        capacity,
        n_fs // n_tp,
    )
    later_chunks = start_later(
        later, later_rows, pltpu.with_memory_space_constraint(gain, pltpu.HBM), weights
    )
    local = dict(zip(early + later, list(early_chunks) + list(later_chunks)))
    chunks = [swap_fs(local[s], s) for s in range(n_fs)]

    down_parts = cast_rows(down_weight, n_tp)
    down_parts = [swap_tp(down_parts[t], t) for t in range(n_tp)]
    down_local = regroup(down_parts)
    down_chunks = [swap_fs(down_local[s], s) for s in range(n_fs)]

    parts, quarters = [], []
    for k, batch in enumerate(batches):
        rows = slot_rows_of([chunks[s] for s in batch], 2 * block, capacity)
        parts.append(gather_tp(rows) if k == 0 else [swap_tp(rows, t) for t in range(n_tp)])
    for batch in batches:
        pieces = regroup([down_chunks[s] for s in batch])
        quarters.append([swap_tp(pieces[t], t) for t in range(n_tp)])

    hidden = gate_up(parts, chunks, block)
    hiddens = [swap_tp(hidden, t) for t in range(n_tp)]
    rows = down(row_order, hiddens, down_chunks, capacity)
    rows = rows.reshape(n_fs * n_tp, *rows.shape[2:])
    back = lax.all_to_all(rows, ("fs", "tp"), split_axis=0, concat_axis=0, tiled=True)
    gate_out, up_out, down_half = store(chunks, block, batches[0], quarters[0])
    mixed, down_out = finish(info, back, n_fs, batches[1], quarters[1], down_half)
    return gate_out, up_out, down_out, mixed


def halves_of(n_fs):
    steps = [s ^ (n_fs - 1) for s in range(n_fs)]
    return steps[: n_fs // 2], steps[n_fs // 2 :]


def slot_tables(route_ids, experts, capacity):
    row_count = route_ids.shape[0]
    pair_count = 2 * row_count
    flat_ids = route_ids.reshape(pair_count)
    onehot = (flat_ids[:, None] == jnp.arange(experts, dtype=jnp.int32)[None, :]).astype(
        jnp.bfloat16
    )
    positions = jnp.arange(pair_count, dtype=jnp.int32)
    below_mask = (positions[:, None] > positions[None, :]).astype(jnp.bfloat16)
    before = jnp.dot(below_mask, onehot, preferred_element_type=jnp.float32)
    ranked = jnp.sum(before * onehot.astype(jnp.float32), axis=1).astype(jnp.int32)
    return (flat_ids * capacity + ranked).reshape(row_count, 2)


def first_products(slot_rows, gate_cols, up_cols):
    shard_cols = lax.all_gather(slot_rows, "tp", axis=1, tiled=True)
    return (
        jnp.dot(shard_cols, gate_cols, preferred_element_type=jnp.float32),
        jnp.dot(shard_cols, up_cols, preferred_element_type=jnp.float32),
    )


def body(
    tokens, norm_gain, gate_weight, up_weight, down_weight, route_ids, group_weight, logit_gap
):
    experts = gate_weight.shape[0]
    tok_rows = tokens.shape[0]
    capacity = max(2, (3 * tok_rows + experts - 1) // experts)
    folded = norm_gain[None, :, None]
    gate_local = (gate_weight * folded).astype(jnp.bfloat16)
    up_local = (up_weight * folded).astype(jnp.bfloat16)
    down_local = down_weight.astype(jnp.bfloat16)
    slot_ids = slot_tables(route_ids, experts, capacity)
    slot_range = jnp.arange(experts * capacity, dtype=jnp.int32)
    matches = (slot_ids[None, :, :] == slot_range[:, None, None]).astype(jnp.int32)
    dispatch = jnp.sum(matches, axis=2).astype(jnp.bfloat16)
    outgoing = jnp.dot(dispatch, tokens, preferred_element_type=jnp.float32).astype(jnp.bfloat16)
    outgoing = outgoing.reshape(experts, capacity, tokens.shape[1])
    arrived = lax.all_to_all(outgoing, "fs", split_axis=0, concat_axis=0, tiled=True)
    slot_rows = arrived.reshape(experts * capacity, tokens.shape[1])
    gate_out, up_out, down_out = (
        lax.all_to_all(gate_local, "fs", split_axis=0, concat_axis=1, tiled=True),
        lax.all_to_all(up_local, "fs", split_axis=0, concat_axis=1, tiled=True),
        lax.all_to_all(down_local, "fs", split_axis=0, concat_axis=1, tiled=True),
    )
    gate_acc, up_acc = first_products(slot_rows, gate_out[0], up_out[0])
    hidden = (jax.nn.silu(gate_acc) * up_acc).astype(jnp.bfloat16)
    partial_value = lax.dot_general(
        hidden, down_out[0], (((1,), (1,)), ((), ())), preferred_element_type=jnp.float32
    )
    summed = lax.psum_scatter(
        partial_value.astype(jnp.bfloat16), "tp", scatter_dimension=1, tiled=True
    )
    returned = lax.all_to_all(
        summed.reshape(experts, capacity, summed.shape[1]),
        "fs",
        split_axis=0,
        concat_axis=0,
        tiled=True,
    )
    back_rows = returned.reshape(experts * capacity, summed.shape[1])
    pick_first = (slot_ids[:, 0:1] == slot_range[None, :]).astype(jnp.bfloat16)
    pick_second = (slot_ids[:, 1:2] == slot_range[None, :]).astype(jnp.bfloat16)
    first_vals = jnp.dot(pick_first, back_rows, preferred_element_type=jnp.float32)
    second_vals = jnp.dot(pick_second, back_rows, preferred_element_type=jnp.float32)
    first_weight = group_weight * jax.nn.sigmoid(logit_gap)
    second_weight = group_weight * jax.nn.sigmoid(-logit_gap)
    mixed = (first_weight[:, None] * first_vals + second_weight[:, None] * second_vals).astype(
        jnp.bfloat16
    )
    return (gate_out, up_out, down_out, mixed)


def solution(mesh):
    n_fs, n_tp = mesh.shape["fs"], mesh.shape["tp"]
    small = n_fs <= 16 and n_fs % n_tp == 0 and n_fs & (n_fs - 1) == 0

    def step(*args):
        if not small:
            return body(*args)
        return exchange_body(n_fs, n_tp, *args)

    return jax.shard_map(
        step,
        mesh=mesh,
        in_specs=(
            P("fs", "tp"),
            P("fs"),
            P(None, "fs", "tp"),
            P(None, "fs", "tp"),
            P(None, "fs", "tp"),
            P("fs", None),
            P("fs"),
            P("fs"),
        ),
        out_specs=(P("fs", None, "tp"), P("fs", None, "tp"), P("fs", None, "tp"), P("fs", "tp")),
        check_vma=False,
    )
```
